512 devices in a mesh: sp: 64 (over z, y), fs: 4 (over x), tp: 2 (over core).
Axes of the slice: x: 4, y: 8, z: 8, core: 2. Of those that a mesh axis runs over, the one named last changes fastest.
Arguments:
- tokens: bfloat16 [8192, 2048], P(('sp', 'fs', 'tp')), may hold values from -16 to 16
- in_gain: float32 [2048], replicated, may hold values from 0.1 to 1.9
- ret_query: bfloat16 [2048, 1024], P(None, ('fs', 'tp')), may hold values from -0.125 to 0.125
- ret_key: bfloat16 [2048, 1024], P(None, ('fs', 'tp')), may hold values from -0.125 to 0.125
- ret_value: bfloat16 [2048, 1024], P(None, ('fs', 'tp')), may hold values from -0.125 to 0.125
- decay_log: float32 [8, 8192], P(('fs', 'tp'), 'sp'), may hold values from -1 to 0
- init_state: bfloat16 [8, 128, 128], P(('fs', 'tp')), may hold values from -24 to 24
- ret_gain: float32 [1024], P(('fs', 'tp')), may hold values from 0.1 to 1.9
- diff_query: bfloat16 [2, 2048, 512], P(None, None, ('fs', 'tp')), may hold values from -1 to 1
- diff_key: bfloat16 [2, 2048, 512], P(None, None, ('fs', 'tp')), may hold values from -1 to 1
- diff_value: bfloat16 [2048, 1024], P(None, ('fs', 'tp')), may hold values from -0.125 to 0.125
- diff_lambda: float32 [8], P(('fs', 'tp')), may hold values from 0.3 to 0.8
- diff_gain: float32 [1024], P(('fs', 'tp')), may hold values from 0.1 to 1.9
- out_weight: bfloat16 [2, 1024, 2048], P(None, ('fs', 'tp'), 'sp'), may hold values from -0.125 to 0.125
Outputs:
- mixed: bfloat16 [8192, 2048], P(('sp', 'fs', 'tp'))
The draws below stay inside these ranges and needn't reach their ends.
All inputs are finite; a program needn't handle non-finite values.
Results may differ from the reference program's by a relative error of at most 0.017.
Values may be sent and summed in bfloat16 or wider, within the bound.
A program may use at most 64 MiB of HBM per device.

```python
import jax
import jax.numpy as jnp
from jax import lax

D = 2048
KEEPING_MIXERS = 8
DIFF_HEADS = 8
HEAD = 128
MAP = 64
RBLOCK = 128
SHARD_POSITIONS = 128
TOKEN_COUNT = 8192
N_SP = 64


def draw_tokens(key, part):
    sample = jax.random.normal(jax.random.fold_in(key, 11), (TOKEN_COUNT, D), jnp.float32)
    return jnp.clip(sample, -16.0, 16.0).astype(jnp.bfloat16)


def projection_draw(key, salt):
    sample = jax.random.normal(jax.random.fold_in(key, salt), (2, D, DIFF_HEADS * MAP), jnp.float32) * (1.3 * D ** (-0.5))
    return jnp.clip(sample, -1.0, 1.0)


def draw_diff_query(key, part):
    return projection_draw(key, 21).astype(jnp.bfloat16)


def draw_diff_key(key, part):
    return projection_draw(key, 22).astype(jnp.bfloat16)


def draw_decay_log(key, part):
    head_shape = (KEEPING_MIXERS, 1)
    slow_share = 0.5
    slow_heads = jax.random.uniform(jax.random.fold_in(key, 31), head_shape) < slow_share
    fast_rate = jax.random.uniform(jax.random.fold_in(key, 32), head_shape, minval=1.0 / 60.0, maxval=1.0 / 30.0)
    slow_rate = jax.random.uniform(jax.random.fold_in(key, 33), head_shape, minval=0.05, maxval=0.3) / TOKEN_COUNT
    single_tick_fading = jnp.where(slow_heads, slow_rate, fast_rate)
    fading_multiplier = jax.random.uniform(jax.random.fold_in(key, 34), (1, TOKEN_COUNT // SHARD_POSITIONS, 1), minval=1.0, maxval=3.0)
    fading_multiplier = jnp.broadcast_to(fading_multiplier, (1, TOKEN_COUNT // SHARD_POSITIONS, SHARD_POSITIONS)).reshape(1, TOKEN_COUNT)
    spurt_clusters = jax.random.uniform(jax.random.fold_in(key, 35), (KEEPING_MIXERS, TOKEN_COUNT)) < 3.0 / TOKEN_COUNT
    fading_drops = jnp.log(jax.random.uniform(jax.random.fold_in(key, 36), (KEEPING_MIXERS, TOKEN_COUNT), minval=0.5, maxval=0.8))
    return -single_tick_fading * fading_multiplier + jnp.where(spurt_clusters, fading_drops, 0.0)


def level_of(key, extent, shards, smallest, largest):
    def one(axis_at, blocks):
        heights = jax.random.uniform(jax.random.fold_in(jax.random.fold_in(key, 6), axis_at), (blocks,), jnp.float32, smallest / len(shards), largest / len(shards))
        return jnp.repeat(jnp.exp(heights), extent[axis_at] // blocks).reshape((-1,) + (1,) * (len(extent) - axis_at - 1))

    level = one(*shards[0])
    for cut in shards[1:]:
        level = level * one(*cut)
    return level


def normal_values(rng, dims, spread, most, shards=(), kind=jnp.bfloat16):
    values = jax.random.normal(rng, dims, jnp.float32) * spread
    if len(shards) > 0:
        values = level_of(rng, dims, shards, -0.22, 0.18) * values
    return jnp.clip(values, min=-most, max=most).astype(kind)


def setup_inputs(seed: int = 0) -> dict:
    keys = jax.random.split(jax.random.key(seed), 15)
    return {
        "tokens": draw_tokens(jax.random.fold_in(keys[14], 71), 0),
        "in_gain": jnp.clip(1.0 + 0.18 * jax.random.normal(keys[1], (D,), jnp.float32), 0.1, 1.9),
        "ret_query": normal_values(keys[2], (D, KEEPING_MIXERS * HEAD), D ** -0.5, 0.125, ((1, 8),)),
        "ret_key": normal_values(keys[3], (D, KEEPING_MIXERS * HEAD), D ** -0.5, 0.125, ((1, 8),)),
        "ret_value": normal_values(keys[4], (D, KEEPING_MIXERS * HEAD), D ** -0.5, 0.125, ((1, 8),)),
        "decay_log": draw_decay_log(jax.random.fold_in(keys[14], 71), 0),
        "init_state": normal_values(keys[6], (KEEPING_MIXERS, HEAD, HEAD), 4.0, 24.0, ((0, 8),)),
        "ret_gain": jnp.clip(1.0 + 0.18 * jax.random.normal(keys[7], (KEEPING_MIXERS * HEAD,), jnp.float32), 0.1, 1.9),
        "diff_query": draw_diff_query(jax.random.fold_in(keys[14], 71), 0),
        "diff_key": draw_diff_key(jax.random.fold_in(keys[14], 71), 0),
        "diff_value": normal_values(keys[10], (D, DIFF_HEADS * HEAD), D ** -0.5, 0.125, ((1, 8),)),
        "diff_lambda": jnp.clip(0.3 + 0.5 * jax.random.uniform(keys[11], (DIFF_HEADS,), jnp.float32) ** level_of(keys[11], (DIFF_HEADS,), ((0, 8),), -0.2, 0.2), 0.3, 0.8),
        "diff_gain": jnp.clip(1.0 + 0.18 * jax.random.normal(keys[12], (DIFF_HEADS * HEAD,), jnp.float32), 0.1, 1.9),
        "out_weight": normal_values(keys[13], (2, KEEPING_MIXERS * HEAD, D), (2 * KEEPING_MIXERS * HEAD) ** -0.5, 0.125, ((1, 8), (2, 64))),
    }


EPS = 1e-06
HUGE = 1e+30
UPPER_LIMIT = lax.Precision.HIGHEST

def norm_rows(rows, gain):
    widened = rows.astype(jnp.float32)
    fading_multiplier = lax.rsqrt(lax.optimization_barrier(jnp.mean(widened * widened, axis=-1, keepdims=True)) + EPS)
    return (widened * fading_multiplier * gain).astype(jnp.bfloat16)

def split_heads(normed, weight, width):
    result = jnp.dot(normed, weight, preferred_element_type=jnp.float32).astype(jnp.bfloat16)
    return jnp.transpose(result.reshape(1, TOKEN_COUNT, -1, width), (2, 0, 1, 3))

def group_norm(output, gain):
    centre = output - lax.optimization_barrier(jnp.mean(output, axis=-1, keepdims=True))
    fading_multiplier = lax.rsqrt(lax.optimization_barrier(jnp.mean(centre * centre, axis=-1, keepdims=True)) + EPS)
    return (centre * fading_multiplier * gain).astype(jnp.bfloat16)

def retention_head(query_rows, key_rows, value_rows, log_rates, start_state):
    seq_total = query_rows.shape[0]
    head_size = query_rows.shape[2]
    blocks = TOKEN_COUNT // RBLOCK

    def to_blocks(array):
        return jnp.swapaxes(array.reshape((seq_total, blocks, RBLOCK) + array.shape[2:]), 0, 1)
    lower = jnp.arange(RBLOCK)[:, None] >= jnp.arange(RBLOCK)[None, :]

    def advance(carried_state, inputs):
        block_queries, block_keys, block_values, block_rates = inputs
        cumulative_decay = jnp.cumsum(block_rates, axis=-1)
        gaps = jnp.where(lower, cumulative_decay[:, :, None] - cumulative_decay[:, None, :], -HUGE)
        widened_queries = block_queries.astype(jnp.float32)
        keys_wide = block_keys.astype(jnp.float32)
        widened_values = block_values.astype(jnp.float32)
        scores = jnp.einsum('sik,sjk->sij', widened_queries, keys_wide) * head_size ** (-0.5) * jnp.exp(gaps)
        rounded = lax.optimization_barrier(scores.astype(jnp.bfloat16)).astype(jnp.float32)
        inner = jnp.einsum('sij,sjv->siv', rounded, widened_values)
        reached_length = jnp.einsum('wny,wyo->wno', widened_queries * jnp.exp(cumulative_decay)[:, :, None], carried_state, precision=UPPER_LIMIT)
        ending_index = cumulative_decay[:, -1]
        weighted_values = keys_wide * (jnp.exp(ending_index[:, None] - cumulative_decay) * head_size ** (-0.5))[:, :, None]
        carried_state = jnp.exp(ending_index)[:, None, None] * carried_state + jnp.einsum('bdg,bdl->bgl', weighted_values, widened_values, precision=UPPER_LIMIT)
        return (carried_state, inner + reached_length)
    _, output = lax.scan(advance, start_state, (to_blocks(query_rows), to_blocks(key_rows), to_blocks(value_rows), to_blocks(log_rates)))
    return jnp.swapaxes(output, 0, 1).reshape(seq_total, TOKEN_COUNT, head_size)

def absorb(running, query_rows, key_rows, value_rows, allowed):
    peak_old, total_old, sum_old = running
    scores = jnp.einsum('...qd,...kd->...qk', query_rows.astype(jnp.float32), key_rows.astype(jnp.float32)) * query_rows.shape[-1] ** (-0.5)
    if allowed is not None:
        scores = jnp.where(allowed, scores, -HUGE)
    block_peak = lax.optimization_barrier(jnp.max(scores, axis=-1))
    weights = jnp.exp(scores - block_peak[..., None])
    block_total = lax.optimization_barrier(jnp.sum(weights, axis=-1))
    rounded = lax.optimization_barrier(weights.astype(jnp.bfloat16)).astype(jnp.float32)
    block_sum = jnp.einsum('...qk,...kv->...qv', rounded, value_rows.astype(jnp.float32))
    new_peak = jnp.maximum(peak_old, block_peak)
    before = jnp.exp(peak_old - new_peak)
    after = jnp.exp(block_peak - new_peak)
    return (new_peak, total_old * before + block_total * after, sum_old * before[..., None] + block_sum * after[..., None])

def diff_head(first_query, second_query, first_key, second_key, value_rows, lambda_head, gain):
    seq_total = first_query.shape[0]
    blocks = N_SP

    def as_blocks(array):
        return array.reshape(seq_total, blocks, SHARD_POSITIONS, array.shape[-1])
    within = jnp.arange(SHARD_POSITIONS)[:, None] >= jnp.arange(SHARD_POSITIONS)[None, :]
    queries = (as_blocks(first_query), as_blocks(second_query))
    key_sets = (as_blocks(first_key), as_blocks(second_key))
    values = as_blocks(value_rows)
    results = []
    for branch in range(2):
        running = (jnp.full((seq_total, blocks, SHARD_POSITIONS), -HUGE, jnp.float32), jnp.zeros((seq_total, blocks, SHARD_POSITIONS), jnp.float32), jnp.zeros((seq_total, blocks, SHARD_POSITIONS, values.shape[-1]), jnp.float32))
        for distance in range(blocks):
            allowed = within if distance == 0 else None
            fresh = absorb(tuple((member[:, distance:] for member in running)), queries[branch][:, distance:], key_sets[branch][:, :blocks - distance], values[:, :blocks - distance], allowed)
            running = tuple((member.at[:, distance:].set(update) for member, update in zip(running, fresh)))
        results.append(running)
    mixed = results[0][2] / results[0][1][..., None] - lambda_head * results[1][2] / results[1][1][..., None]
    mixed = mixed.reshape(seq_total, TOKEN_COUNT, -1)
    fading_multiplier = lax.rsqrt(lax.optimization_barrier(jnp.mean(mixed * mixed, axis=-1, keepdims=True)) + EPS)
    return (mixed * fading_multiplier * gain).astype(jnp.bfloat16)

def reference(tokens, in_gain, ret_query, ret_key, ret_value, decay_log, init_state, ret_gain, diff_query, diff_key, diff_value, diff_lambda, diff_gain, out_weight):
    normed = norm_rows(tokens, in_gain)
    ret_queries = split_heads(normed, ret_query, HEAD)
    ret_keys = split_heads(normed, ret_key, HEAD)
    ret_values = split_heads(normed, ret_value, HEAD)
    first_query = split_heads(normed, diff_query[0], MAP)
    second_query = split_heads(normed, diff_query[1], MAP)
    first_key = split_heads(normed, diff_key[0], MAP)
    second_key = split_heads(normed, diff_key[1], MAP)
    diff_values = split_heads(normed, diff_value, HEAD)
    rates = decay_log.reshape(KEEPING_MIXERS, 1, TOKEN_COUNT)
    starts = init_state.astype(jnp.float32).reshape(KEEPING_MIXERS, 1, HEAD, HEAD)

    def retention_item(head_items):
        output = retention_head(head_items[0], head_items[1], head_items[2], head_items[3], head_items[4])
        return group_norm(output, head_items[5])
    ret_mix = lax.map(retention_item, (ret_queries, ret_keys, ret_values, rates, starts, ret_gain.reshape(KEEPING_MIXERS, HEAD)))

    def diff_item(head_items):
        return diff_head(head_items[0], head_items[1], head_items[2], head_items[3], head_items[4], head_items[5], head_items[6])
    diff_mix = lax.map(diff_item, (first_query, second_query, first_key, second_key, diff_values, diff_lambda, diff_gain.reshape(DIFF_HEADS, HEAD)))
    ret_rows = out_weight[0].reshape(KEEPING_MIXERS, HEAD, D)
    diff_rows = out_weight[1].reshape(DIFF_HEADS, HEAD, D)

    def add_head(running_total, head_items):
        ret_part, diff_part, ret_weight, diff_weight = head_items
        partial_value = jnp.dot(ret_part.reshape(-1, HEAD), ret_weight, preferred_element_type=jnp.float32)
        partial_value = partial_value + jnp.dot(diff_part.reshape(-1, HEAD), diff_weight, preferred_element_type=jnp.float32)
        return (running_total + lax.optimization_barrier(partial_value.astype(jnp.bfloat16)).astype(jnp.float32), None)
    summed, _ = lax.scan(add_head, jnp.zeros((TOKEN_COUNT, D), jnp.float32), (ret_mix, diff_mix, ret_rows, diff_rows))
    return summed.astype(jnp.bfloat16)
```

```python
import functools

import jax
import jax.numpy as jnp
from jax import lax
from jax.experimental import pallas as pl
from jax.experimental.pallas import tpu as pltpu
from jax.sharding import Mesh
from jax.sharding import PartitionSpec as P

SP = ("sp_0", "sp_1")
SP_FS_TP = ("sp_0", "sp_1", "fs", "tp")
MESH = pl.DeviceIdType.MESH
EPS = 1e-06
HUGE = 1e30
FLOOR = -1e29
BLK = 128
BF = jnp.bfloat16
F32 = jnp.float32
HIGH = lax.Precision.HIGHEST


def dot(a, b, **kw):
    return jnp.dot(a, b, preferred_element_type=F32, **kw)


def dot_nt(a, b):
    return lax.dot_general(a, b, (((1,), (1,)), ((), ())), preferred_element_type=F32)


def iota(shape, dim):
    return lax.broadcasted_iota(jnp.int32, shape, dim)


def kernel(
    dims,
    tok_h, gain_h, wrq_h, wrk_h, wrv_h, dec_h, init_h, rgain_h, wq_h, wk_h, wv_h, lam_s, dgain_h, ow_h,
    out_ref,
    tok, gain, dec, init, rgain, dgain, wqk, w, x,
    kall, vtall, qbuf, so, st, ro, rst,
    sa, sda, ra, rda, sb, sdb, rb, rdb, sc, rc,
    wsm, wbig, fs, fr,
    in_sem, tok_ss, tok_rs, ow_ss, ow_rs, kf_ss, kf_rs, kb_ss, kb_rs, q_ss, q_rs,
    a_ss, a_rs, b_ss, b_rs, c_ss, c_rs, r_ss, r_rs, wf_ss, wf_rs, wb_ss, wb_rs, f_ss, f_rs,
):
    nz, ny, nx, nc = dims
    nh = nx * nc
    rows = BLK // nh
    sl = BLK // ny
    nf, nb = nz // 2, nz - 1 - nz // 2
    z, y = lax.axis_index("sp_0"), lax.axis_index("sp_1")
    fx, c = lax.axis_index("fs"), lax.axis_index("tp")
    h = fx * nc + c

    def head_peer(d):
        p = lax.rem(h + d, nh)
        return p, (z, y, p // nc, lax.rem(p, nc))

    def y_peer(d):
        p = lax.rem(y + d, ny)
        return p, (z, p, fx, c)

    def z_peer(d):
        p = lax.rem(z + d, nz)
        return p, (p, y, fx, c)

    def rcopy(src, dst, ss, rs, dev):
        return pltpu.make_async_remote_copy(
            src_ref=src, dst_ref=dst, send_sem=ss, recv_sem=rs, device_id=dev, device_id_type=MESH
        )

    barrier = pltpu.get_barrier_semaphore()
    for d in range(1, nh):
        pl.semaphore_signal(barrier, inc=1, device_id=head_peer(d)[1], device_id_type=MESH)
    for d in range(1, ny):
        pl.semaphore_signal(barrier, inc=1, device_id=y_peer(d)[1], device_id_type=MESH)
    for d in range(1, nz):
        pl.semaphore_signal(barrier, inc=1, device_id=z_peer(d)[1], device_id_type=MESH)

    own_w = wsm.at[:, pl.ds(pl.multiple_of(y * 32, 32), 32), :]
    inputs = [
        (tok_h, tok), (gain_h, gain), (ow_h, own_w), (wk_h, wqk.at[0]), (wq_h, wqk.at[1]),
        (wv_h, w.at[:, pl.ds(128, 128)]), (wrq_h, w.at[:, pl.ds(384, 128)]),
        (wrk_h, w.at[:, pl.ds(512, 128)]), (wrv_h, w.at[:, pl.ds(640, 128)]),
        (dec_h, dec), (init_h, init), (rgain_h, rgain), (dgain_h, dgain),
    ]
    loads = [pltpu.make_async_copy(s, t, in_sem.at[i]) for i, (s, t) in enumerate(inputs)]
    for copy in loads:
        copy.start()

    loads[0].wait()
    loads[1].wait()
    t = tok[...].astype(F32)
    scale = lax.rsqrt(jnp.mean(t * t, axis=-1, keepdims=True) + EPS)
    own_x = x.at[pl.ds(pl.multiple_of(h * rows, rows), rows), :]
    own_x[...] = (t * scale * gain[...]).astype(BF)
    loads[2].wait()

    pl.semaphore_wait(barrier, nh + ny + nz - 3)

    sends = []

    def go(copy):
        copy.start()
        sends.append(copy)

    for d in range(1, nh):
        go(rcopy(own_x, own_x, tok_ss.at[d], tok_rs.at[d], head_peer(d)[1]))
    for d in range(1, ny):
        go(rcopy(own_w, own_w, ow_ss.at[d], ow_rs.at[d], y_peer(d)[1]))

    loads[3].wait()
    w[:, 0:128] = wqk[0].astype(F32).T.astype(BF)
    loads[4].wait()
    w[:, 256:384] = wqk[1].astype(F32).T.astype(BF)
    for copy in loads[5:]:
        copy.wait()

    row, col = iota((BLK, BLK), 0), iota((BLK, BLK), 1)
    lower = row >= col
    decb = jnp.broadcast_to(dec[...], (BLK, BLK))
    cum_col = jnp.sum(jnp.where(lower, decb, 0.0), axis=1, keepdims=True)
    dec_col = jnp.sum(jnp.where(row == col, decb, 0.0), axis=1, keepdims=True)
    cum_row = jnp.sum(jnp.where(row <= col, jnp.broadcast_to(dec_col, (BLK, BLK)), 0.0), axis=0, keepdims=True)
    cum_end = jnp.sum(dec[...], axis=1, keepdims=True)
    fade = jnp.exp(jnp.where(lower, cum_col - cum_row, -HUGE)) * (BLK ** (-0.5))
    key_weight = jnp.exp(cum_end - cum_col) * (BLK ** (-0.5))
    reach = jnp.exp(cum_col)
    sda[...] = jnp.broadcast_to(jnp.exp(cum_end), sda.shape)

    for d in range(1, nh):
        p, dev = head_peer(nh - d)
        part = x.at[pl.ds(pl.multiple_of(p * rows, rows), rows), :]
        rcopy(part, part, tok_ss.at[d], tok_rs.at[d], dev).wait_recv()

    xs = x[...]
    kv = dot(xs, w[:, 0:256])
    kall[0:BLK, :] = kv[:, 0:128].astype(BF)
    vtall[:, 0:BLK] = kv[:, 128:256].T.astype(BF)

    def k_at(s):
        return kall.at[pl.ds(s * BLK, BLK), :]

    def v_at(s):
        return vtall.at[:, pl.ds(s * BLK, BLK)]

    right, left = z_peer(1)[1], z_peer(nz - 1)[1]

    def kv_hop(s, forward, part):
        if forward:
            src, dst, ss, rs, dev = s - 1, s, kf_ss, kf_rs, right
        else:
            src, dst, ss, rs, dev = (0 if s == 1 else nf + s - 1), nf + s, kb_ss, kb_rs, left
        at = (k_at, v_at)[part]
        return rcopy(at(src), at(dst), ss.at[s - 1, part], rs.at[s - 1, part], dev)

    def kv_start(s):
        for part in range(2):
            if s <= nf:
                go(kv_hop(s, True, part))
            if s <= nb:
                go(kv_hop(s, False, part))

    def kv_advance(s):
        for part in range(2):
            if s <= nf:
                kv_hop(s, True, part).wait_recv()
                if s + 1 <= nf:
                    go(kv_hop(s + 1, True, part))
            if s <= nb:
                kv_hop(s, False, part).wait_recv()
                if s + 1 <= nb:
                    go(kv_hop(s + 1, False, part))

    kv_start(1)

    rest = dot(xs, w[:, 256:768])
    qbuf[0] = (rest[:, 0:128].astype(BF).astype(F32) * (64 ** (-0.5))).T.astype(BF)
    for d in range(1, ny):
        go(rcopy(qbuf.at[0], qbuf.at[d], q_ss.at[d], q_rs.at[d], y_peer(d)[1]))

    rq, rk, rv = (rest[:, 128 * i : 128 * (i + 1)].astype(BF) for i in (1, 2, 3))
    keyed = (rk.astype(F32) * key_weight).T
    state = dot(keyed, rv.astype(F32), precision=HIGH)
    sa[...] = state.reshape(ny, sl, BLK)
    ra[pl.ds(y, 1)] = sa[pl.ds(y, 1)]
    rda[pl.ds(y, 1)] = sda[...].reshape(1, 1, BLK)
    for d in range(1, ny):
        p, dev = y_peer(d)
        go(rcopy(sa.at[p], ra.at[y], a_ss.at[d, 0], a_rs.at[d, 0], dev))
        go(rcopy(sda, rda.at[y], a_ss.at[d, 1], a_rs.at[d, 1], dev))

    kv_advance(1)
    scores = dot_nt(rq, rk) * fade
    inner = dot(scores.astype(BF), rv)
    reaching = rq.astype(F32) * reach

    kv_advance(2)

    for d in range(1, ny):
        p, dev = y_peer(ny - d)
        part = wsm.at[:, pl.ds(pl.multiple_of(p * 32, 32), 32), :]
        rcopy(part, part, ow_ss.at[d], ow_rs.at[d], dev).wait_recv()
    for i in range(2):
        wbig[pl.ds(z, 1), i * 128 : (i + 1) * 128, :] = wsm[i].astype(F32).T.astype(BF)[None]

    for s in range(3, nf):
        kv_advance(s)

    for d in range(1, ny):
        p, dev = y_peer(ny - d)
        rcopy(sa.at[p], ra.at[p], a_ss.at[d, 0], a_rs.at[d, 0], dev).wait_recv()
        rcopy(sda, rda.at[p], a_ss.at[d, 1], a_rs.at[d, 1], dev).wait_recv()
    total = ra[0]
    decay = rda[0]
    for i in range(1, ny):
        total = rda[i] * total + ra[i]
        decay = decay * rda[i]
    sb[...] = total
    sdb[...] = decay
    rb[pl.ds(z, 1)] = jnp.zeros((1, sl, BLK), F32)
    rdb[pl.ds(z, 1)] = jnp.zeros((1, 1, BLK), F32)
    for d in range(1, nz):
        dev = z_peer(d)[1]
        go(rcopy(sb, rb.at[z], b_ss.at[d, 0], b_rs.at[d, 0], dev))
        go(rcopy(sdb, rdb.at[z], b_ss.at[d, 1], b_rs.at[d, 1], dev))

    if nf > 2:
        kv_advance(nf)

    def ow_hop(s, half, forward):
        if forward:
            slot, ss, rs, dev = lax.rem(z + nz - s + 1, nz), wf_ss, wf_rs, right
        else:
            slot, ss, rs, dev = lax.rem(z + s - 1, nz), wb_ss, wb_rs, left
        ref = wbig.at[slot, pl.ds(half * 128, 128), :]
        return rcopy(ref, ref, ss.at[s - 1, half], rs.at[s - 1, half], dev)

    def ow_wait(s, half, forward):
        if forward:
            slot, ss, rs, dev = lax.rem(z + nz - s, nz), wf_ss, wf_rs, right
        else:
            slot, ss, rs, dev = lax.rem(z + s, nz), wb_ss, wb_rs, left
        ref = wbig.at[slot, pl.ds(half * 128, 128), :]
        rcopy(ref, ref, ss.at[s - 1, half], rs.at[s - 1, half], dev).wait_recv()

    def ow_start(s):
        for half in range(2):
            if s <= nf:
                go(ow_hop(s, half, True))
            if s <= nb:
                go(ow_hop(s, half, False))

    def ow_advance(s):
        for half in range(2):
            if s <= nf:
                ow_wait(s, half, True)
                if s + 1 <= nf:
                    go(ow_hop(s + 1, half, True))
            if s <= nb:
                ow_wait(s, half, False)
                if s + 1 <= nb:
                    go(ow_hop(s + 1, half, False))

    ow_start(1)

    for d in range(1, ny):
        rcopy(qbuf.at[0], qbuf.at[d], q_ss.at[d], q_rs.at[d], y_peer(ny - d)[1]).wait_recv()

    def finish_states():
        for d in range(1, nz):
            p, dev = z_peer(nz - d)
            rcopy(sb, rb.at[p], b_ss.at[d, 0], b_rs.at[d, 0], dev).wait_recv()
            rcopy(sdb, rdb.at[p], b_ss.at[d, 1], b_rs.at[d, 1], dev).wait_recv()
        entry = init[0, pl.ds(pl.multiple_of(y * sl, sl), sl), :].astype(F32)
        for i in range(nz):
            entry = jnp.where(i < z, rdb[i] * entry + rb[i], entry)
        for i in range(ny):
            sc[i] = entry
            entry = rda[i] * entry + ra[i]
        rc[pl.ds(y, 1)] = sc[pl.ds(y, 1)]
        for d in range(1, ny):
            p, dev = y_peer(d)
            rcopy(sc.at[p], rc.at[y], c_ss.at[d], c_rs.at[d], dev).start()

    krow, lane = iota((BLK, 2 * BLK), 0), iota((BLK, 2 * BLK), 1)
    qlane = jnp.where(lane >= BLK, lane - BLK, lane)
    valid = [None] + [jnp.where(s <= z, 0.0, -HUGE) for s in range(1, nf + 1)]
    valid += [jnp.where(z + s >= nz, 0.0, -HUGE) for s in range(1, nb + 1)]

    def attend(i, _):
        k = (i + 1) // 2
        d = lax.rem(ny // 2 + (2 * lax.rem(i, 2) - 1) * k + 2 * ny, ny)
        yq = lax.rem(y - d + ny, ny)
        q = qbuf[d]
        zero = jnp.zeros_like(q)
        top_half = row < 64
        qt = jnp.concatenate([jnp.where(top_half, q, zero), jnp.where(top_half, zero, q)], axis=1)
        s = dot(kall[...], qt)
        pieces = [jnp.where(krow + y * BLK <= qlane + yq * BLK, s[0:BLK], -HUGE)]
        for n in range(1, nz):
            pieces.append(s[n * BLK : (n + 1) * BLK] + valid[n])
        s = jnp.concatenate(pieces, axis=0)
        peak = jnp.maximum(jnp.max(s, axis=0, keepdims=True), FLOOR)
        p = jnp.exp(s - peak)
        st[pl.ds(d, 1), 0:1, :] = peak[None]
        st[pl.ds(d, 1), 1:2, :] = jnp.sum(p, axis=0, keepdims=True)[None]
        so[pl.ds(d, 1)] = dot(vtall[...], p.astype(BF)).astype(BF)[None]

        @pl.when(i < ny - 1)
        def _():
            dev = (z, yq, fx, c)
            rcopy(so.at[d], ro.at[d], r_ss.at[d, 0], r_rs.at[d, 0], dev).start()
            rcopy(st.at[d], rst.at[d], r_ss.at[d, 1], r_rs.at[d, 1], dev).start()

        @pl.when(i == ny // 2)
        def _():
            finish_states()

        return 0

    lax.fori_loop(0, ny, attend, 0)

    for s in range(1, nf + 1):
        ow_advance(s)

    for d in range(1, ny):
        p, dev = y_peer(ny - d)
        rcopy(sc.at[p], rc.at[p], c_ss.at[d], c_rs.at[d], dev).wait_recv()
    ret = inner + dot(reaching, rc[...].reshape(BLK, BLK), precision=HIGH)
    centre = ret - jnp.mean(ret, axis=-1, keepdims=True)
    ret_mix = (
        centre * lax.rsqrt(jnp.mean(centre * centre, axis=-1, keepdims=True) + EPS) * rgain[...]
    ).astype(BF)

    for d in range(1, ny):
        dev = y_peer(d)[1]
        rcopy(so.at[d], ro.at[d], r_ss.at[d, 0], r_rs.at[d, 0], dev).wait_recv()
        rcopy(st.at[d], rst.at[d], r_ss.at[d, 1], r_rs.at[d, 1], dev).wait_recv()
    stats = [st[0]] + [rst[d] for d in range(1, ny)]
    top = stats[0][0:1]
    for one in stats[1:]:
        top = jnp.maximum(top, one[0:1])
    total = jnp.zeros_like(top)
    merged = jnp.zeros((BLK, 2 * BLK), F32)
    for d in range(ny):
        share = jnp.exp(stats[d][0:1] - top)
        total = total + share * stats[d][1:2]
        merged = merged + (so[0] if d == 0 else ro[d]).astype(F32) * share
    merged = merged / total
    diff = merged[:, 0:128] - lam_s[0] * merged[:, 128:256]
    diff = diff * lax.rsqrt(jnp.mean(diff * diff, axis=0, keepdims=True) + EPS)
    diff_mix = (diff.T * dgain[...]).astype(BF)

    mix = jnp.concatenate([ret_mix, diff_mix], axis=1)
    wide = wbig.shape[2]
    for i in range(nz):
        fs[:, i * wide : (i + 1) * wide] = dot(mix, wbig[i]).astype(BF)
    for d in range(1, nh):
        p, dev = head_peer(d)
        part = fs.at[pl.ds(pl.multiple_of(p * rows, rows), rows), :]
        go(rcopy(part, fr.at[d], f_ss.at[d], f_rs.at[d], dev))
    acc = fs[pl.ds(pl.multiple_of(h * rows, rows), rows), :].astype(F32)
    for d in range(1, nh):
        dev = head_peer(d)[1]
        rcopy(own_x, fr.at[d], f_ss.at[d], f_rs.at[d], dev).wait_recv()
        acc = acc + fr[d].astype(F32)
    out_ref[...] = acc.astype(BF)

    for copy in sends:
        copy.wait_send()
    for d in range(1, ny):
        p, dev = y_peer(d)
        rcopy(sc.at[p], rc.at[y], c_ss.at[d], c_rs.at[d], dev).wait_send()
        rcopy(so.at[d], ro.at[d], r_ss.at[d, 0], r_rs.at[d, 0], dev).wait_send()
        rcopy(st.at[d], rst.at[d], r_ss.at[d, 1], r_rs.at[d, 1], dev).wait_send()


def local(
    dims, tokens, in_gain, ret_query, ret_key, ret_value, decay_log, init_state, ret_gain,
    diff_query, diff_key, diff_value, diff_lambda, diff_gain, out_weight,
):
    nz, ny, nx, nc = dims
    nh = nx * nc
    rows, width = tokens.shape
    sl = BLK // ny
    nf, nb = nz // 2, nz - 1 - nz // 2
    dma = pltpu.SemaphoreType.DMA
    vm = pltpu.VMEM
    scratch = [
        vm((rows, width), BF), vm((1, width), F32), vm((1, BLK), F32), vm((1, BLK, BLK), BF),
        vm((1, BLK), F32), vm((1, BLK), F32), vm((2, BLK, width), BF), vm((width, 768), BF), vm((BLK, width), BF),
        vm((nz * BLK, BLK), BF), vm((BLK, nz * BLK), BF), vm((ny, BLK, BLK), BF),
        vm((ny, BLK, 2 * BLK), BF), vm((ny, 2, 2 * BLK), F32), vm((ny, BLK, 2 * BLK), BF), vm((ny, 2, 2 * BLK), F32),
        vm((ny, sl, BLK), F32), vm((1, BLK), F32), vm((ny, sl, BLK), F32), vm((ny, 1, BLK), F32),
        vm((sl, BLK), F32), vm((1, BLK), F32), vm((nz, sl, BLK), F32), vm((nz, 1, BLK), F32),
        vm((ny, sl, BLK), F32), vm((ny, sl, BLK), F32),
        vm((2, 32 * ny, BLK), BF), vm((nz, 2 * BLK, 32 * ny), BF), vm((BLK, width), BF), vm((nh, rows, width), BF),
        dma((13,)), dma((nh,)), dma((nh,)), dma((ny,)), dma((ny,)),
        dma((nf, 2)), dma((nf, 2)), dma((max(nb, 1), 2)), dma((max(nb, 1), 2)), dma((ny,)), dma((ny,)),
        dma((ny, 2)), dma((ny, 2)), dma((nz, 2)), dma((nz, 2)), dma((ny,)), dma((ny,)),
        dma((ny, 2)), dma((ny, 2)), dma((nf, 2)), dma((nf, 2)), dma((max(nb, 1), 2)), dma((max(nb, 1), 2)),
        dma((nh,)), dma((nh,)),
    ]
    anyspec = pl.BlockSpec(memory_space=pl.ANY)
    smem = pl.BlockSpec(memory_space=pltpu.SMEM)
    return pl.pallas_call(
        functools.partial(kernel, dims),
        out_shape=jax.ShapeDtypeStruct((rows, width), BF),
        in_specs=[anyspec] * 11 + [smem] + [anyspec] * 2,
        out_specs=pl.BlockSpec(memory_space=pltpu.VMEM),
        scratch_shapes=scratch,
        compiler_params=pltpu.CompilerParams(
            collective_id=0, has_side_effects=True, vmem_limit_bytes=60 * 1024 * 1024
        ),
    )(
        tokens,
        in_gain.reshape(1, width),
        ret_query,
        ret_key,
        ret_value,
        decay_log,
        init_state,
        ret_gain.reshape(1, BLK),
        jnp.swapaxes(diff_query, 1, 2).reshape(BLK, width),
        jnp.swapaxes(diff_key, 1, 2).reshape(BLK, width),
        diff_value,
        diff_lambda,
        diff_gain.reshape(1, BLK),
        jnp.swapaxes(out_weight, 1, 2),
    )


def build(split):
    dims = tuple(split.shape[a] for a in SP_FS_TP)
    placed = (
        P(SP_FS_TP, None),
        P(),
        P(None, ("fs", "tp")),
        P(None, ("fs", "tp")),
        P(None, ("fs", "tp")),
        P(("fs", "tp"), SP),
        P(("fs", "tp"), None, None),
        P(("fs", "tp")),
        P(None, None, ("fs", "tp")),
        P(None, None, ("fs", "tp")),
        P(None, ("fs", "tp")),
        P(("fs", "tp")),
        P(("fs", "tp")),
        P(None, ("fs", "tp"), SP),
    )
    return jax.shard_map(
        functools.partial(local, dims), mesh=split, in_specs=placed, out_specs=P(SP_FS_TP, None), check_vma=False
    )


def solution(mesh):
    return build(Mesh(mesh.devices.reshape(8, 8, mesh.shape["fs"], mesh.shape["tp"]), SP_FS_TP))
```

```python
import functools

import jax
import jax.numpy as jnp
from jax import lax
from jax.experimental import pallas as pl
from jax.experimental.pallas import tpu as pltpu
from jax.sharding import Mesh
from jax.sharding import PartitionSpec as P

SP = ("sp_0", "sp_1")
SP_FS_TP = ("sp_0", "sp_1", "fs", "tp")
MESH = pl.DeviceIdType.MESH
EPS = 1e-06
HUGE = 1e30
FLOOR = -1e29
BLK = 128
BF = jnp.bfloat16
F32 = jnp.float32
HIGH = lax.Precision.HIGHEST


def dot(a, b, **kw):
    return jnp.dot(a, b, preferred_element_type=F32, **kw)


def dot_nt(a, b):
    return lax.dot_general(a, b, (((1,), (1,)), ((), ())), preferred_element_type=F32)


def iota(shape, dim):
    return lax.broadcasted_iota(jnp.int32, shape, dim)


def kernel(
    dims,
    tok_h, gain_h, wrq_h, wrk_h, wrv_h, dec_h, init_h, rgain_h, wq_h, wk_h, wv_h, lam_s, dgain_h, ow_h,
    out_ref,
    tok, gain, dec, init, rgain, dgain, wqk, w, x,
    kall, vtall, qbuf, so, st, ro, rst,
    sa, sda, ra, rda, sb, sdb, rb, rdb, sc, rc,
    early_sum, early_stat, wt, pwt, wpair, mixb, pmix, fs, fr,
    in_sem, tok_ss, tok_rs, pt_ss, pt_rs, ow_ss, ow_rs, kf_ss, kf_rs, kb_ss, kb_rs, q_ss, q_rs,
    a_ss, a_rs, b_ss, b_rs, c_ss, c_rs, r_ss, r_rs, wf_ss, wf_rs, wb_ss, wb_rs, pw_ss, pw_rs, mix_ss, mix_rs, f_ss, f_rs,
):
    nz, ny, nx, nc = dims
    nh = nx * nc
    rows = BLK // nh
    sl = BLK // ny
    nf, nb = nz // 2, nz - 1 - nz // 2
    early = 5 if nz > 5 else 3
    z, y = lax.axis_index("sp_0"), lax.axis_index("sp_1")
    fx, c = lax.axis_index("fs"), lax.axis_index("tp")
    h = fx * nc + c

    def head_peer(d):
        p = lax.rem(h + d, nh)
        return p, (z, y, p // nc, lax.rem(p, nc))

    a, b = (1 - c) * z + c * y, (1 - c) * y + c * z

    def a_place(p):
        return z + (1 - c) * (p - a), y + c * (p - a)

    def b_place(p):
        return z + c * (p - b), y + (1 - c) * (p - b)

    def a_peer(d):
        return (*a_place(lax.rem(a + d, nz)), fx, c)

    def b_peer(d):
        return (*b_place(lax.rem(b + d, nz)), fx, c)

    def x_peer(d):
        p = lax.rem(fx + d, nx)
        return p, (z, y, p, c)

    partner = (z, y, fx, 1 - c)

    def y_peer(d):
        p = lax.rem(y + d, ny)
        return p, (z, p, fx, c)

    def z_peer(d):
        p = lax.rem(z + d, nz)
        return p, (p, y, fx, c)

    def rcopy(src, dst, ss, rs, dev):
        return pltpu.make_async_remote_copy(
            src_ref=src, dst_ref=dst, send_sem=ss, recv_sem=rs, device_id=dev, device_id_type=MESH
        )

    barrier = pltpu.get_barrier_semaphore()
    for d in range(1, nh):
        pl.semaphore_signal(barrier, inc=1, device_id=head_peer(d)[1], device_id_type=MESH)
    for d in range(1, ny):
        pl.semaphore_signal(barrier, inc=1, device_id=y_peer(d)[1], device_id_type=MESH)
    for d in range(1, nz):
        pl.semaphore_signal(barrier, inc=1, device_id=z_peer(d)[1], device_id_type=MESH)

    inputs = [
        (tok_h, tok), (gain_h, gain), (ow_h, wt.at[:, z, y]), (wk_h, wqk.at[0]), (wq_h, wqk.at[1]),
        (wv_h, w.at[:, pl.ds(128, 128)]), (wrq_h, w.at[:, pl.ds(384, 128)]),
        (wrk_h, w.at[:, pl.ds(512, 128)]), (wrv_h, w.at[:, pl.ds(640, 128)]),
        (dec_h, dec), (init_h, init), (rgain_h, rgain), (dgain_h, dgain),
    ]
    loads = [pltpu.make_async_copy(s, t, in_sem.at[i]) for i, (s, t) in enumerate(inputs)]
    for copy in loads:
        copy.start()

    loads[0].wait()
    loads[1].wait()
    t = tok[...].astype(F32)
    scale = lax.rsqrt(jnp.mean(t * t, axis=-1, keepdims=True) + EPS)
    own_x = x.at[pl.ds(pl.multiple_of(h * rows, rows), rows), :]
    own_x[...] = (t * scale * gain[...]).astype(BF)
    loads[2].wait()

    pl.semaphore_wait(barrier, nh + ny + nz - 3)

    sends = []

    def go(copy):
        copy.start()
        sends.append(copy)

    def x_rows(p, core):
        return x.at[pl.ds(pl.multiple_of((p * nc + core) * rows, rows), rows), :]

    for d in range(1, nx):
        go(rcopy(own_x, own_x, tok_ss.at[d], tok_rs.at[d], x_peer(d)[1]))
    if nc > 1:
        go(rcopy(own_x, own_x, pt_ss.at[0], pt_rs.at[0], partner))
    for d in range(1, ny):
        part = wt.at[0, z, y]
        go(rcopy(part, part, ow_ss.at[d, 0], ow_rs.at[d, 0], y_peer(d)[1]))
        part = wt.at[1, z, y]
        go(rcopy(part, part, ow_ss.at[d, 1], ow_rs.at[d, 1], z_peer(d)[1]))

    loads[3].wait()
    w[:, 0:128] = wqk[0].astype(F32).T.astype(BF)
    loads[4].wait()
    w[:, 256:384] = wqk[1].astype(F32).T.astype(BF)
    for copy in loads[5:]:
        copy.wait()

    row, col = iota((BLK, BLK), 0), iota((BLK, BLK), 1)
    lower = row >= col
    decb = jnp.broadcast_to(dec[...], (BLK, BLK))
    cum_col = jnp.sum(jnp.where(lower, decb, 0.0), axis=1, keepdims=True)
    dec_col = jnp.sum(jnp.where(row == col, decb, 0.0), axis=1, keepdims=True)
    cum_row = jnp.sum(jnp.where(row <= col, jnp.broadcast_to(dec_col, (BLK, BLK)), 0.0), axis=0, keepdims=True)
    cum_end = jnp.sum(dec[...], axis=1, keepdims=True)
    fade = jnp.exp(jnp.where(lower, cum_col - cum_row, -HUGE)) * (BLK ** (-0.5))
    key_weight = jnp.exp(cum_end - cum_col) * (BLK ** (-0.5))
    reach = jnp.exp(cum_col)
    sda[...] = jnp.broadcast_to(jnp.exp(cum_end), sda.shape)

    for d in sorted(range(1, nx), key=lambda v: min(v, nx - v)):
        p, dev = x_peer(nx - d)
        part = x_rows(p, c)
        rcopy(part, part, tok_ss.at[d], tok_rs.at[d], dev).wait_recv()
        if nc > 1:
            go(rcopy(part, part, pt_ss.at[d], pt_rs.at[d], partner))
    if nc > 1:
        for d in range(nx):
            part = x_rows(lax.rem(fx + nx - d, nx), 1 - c)
            rcopy(part, part, pt_ss.at[d], pt_rs.at[d], partner).wait_recv()

    xs = x[...]
    kv = dot(xs, w[:, 0:256])
    kall[0:BLK, :] = kv[:, 0:128].astype(BF)
    vtall[:, 0:BLK] = kv[:, 128:256].T.astype(BF)

    def k_at(s):
        return kall.at[pl.ds(s * BLK, BLK), :]

    def v_at(s):
        return vtall.at[:, pl.ds(s * BLK, BLK)]

    right, left = a_peer(1), a_peer(nz - 1)

    def kv_hop(s, forward, part):
        if forward:
            src, dst, ss, rs, dev = max(2 * s - 3, 0), 2 * s - 1, kf_ss, kf_rs, right
        else:
            src, dst, ss, rs, dev = 2 * s - 2, 2 * s, kb_ss, kb_rs, left
        at = (k_at, v_at)[part]
        return rcopy(at(src), at(dst), ss.at[s - 1, part], rs.at[s - 1, part], dev)

    def kv_start(s):
        for part in range(2):
            if s <= nf:
                go(kv_hop(s, True, part))
            if s <= nb:
                go(kv_hop(s, False, part))

    def kv_advance(s):
        for part in range(2):
            if s <= nf:
                kv_hop(s, True, part).wait_recv()
                if s + 1 <= nf:
                    go(kv_hop(s + 1, True, part))
            if s <= nb:
                kv_hop(s, False, part).wait_recv()
                if s + 1 <= nb:
                    go(kv_hop(s + 1, False, part))

    kv_start(1)

    rest = dot(xs, w[:, 256:768])
    qbuf[0] = (rest[:, 0:128].astype(BF).astype(F32) * (64 ** (-0.5))).T.astype(BF)
    for d in range(1, ny):
        go(rcopy(qbuf.at[0], qbuf.at[d], q_ss.at[d], q_rs.at[d], b_peer(d)))

    rq, rk, rv = (rest[:, 128 * i : 128 * (i + 1)].astype(BF) for i in (1, 2, 3))
    keyed = (rk.astype(F32) * key_weight).T
    state = dot(keyed, rv.astype(F32), precision=HIGH)
    sa[...] = state.reshape(ny, sl, BLK)
    ra[pl.ds(y, 1)] = sa[pl.ds(y, 1)]
    rda[pl.ds(y, 1)] = sda[...].reshape(1, 1, BLK)
    for d in range(1, ny):
        p, dev = y_peer(d)
        go(rcopy(sa.at[p], ra.at[y], a_ss.at[d, 0], a_rs.at[d, 0], dev))
        go(rcopy(sda, rda.at[y], a_ss.at[d, 1], a_rs.at[d, 1], dev))

    for d in range(1, ny):
        part = wt.at[0, z, y_peer(ny - d)[0]]
        rcopy(part, part, ow_ss.at[d, 0], ow_rs.at[d, 0], partner).wait_recv()
        part = wt.at[1, z_peer(nz - d)[0], y]
        rcopy(part, part, ow_ss.at[d, 1], ow_rs.at[d, 1], partner).wait_recv()

    def ow_hop(s, half, forward, arriving=False):
        place, peer = ((z, z_peer), (y, y_peer))[half]
        back = s if arriving else s - 1
        slot = lax.rem(place + (nz - back if forward else back), nz)
        ref = wt.at[0, slot] if half == 0 else wt.at[1, :, slot]
        ss, rs = (wf_ss, wf_rs) if forward else (wb_ss, wb_rs)
        return rcopy(ref, ref, ss.at[s - 1, half], rs.at[s - 1, half], peer(1 if forward else nz - 1)[1])

    def ow_start(s):
        for half in range(2):
            if s <= nf:
                go(ow_hop(s, half, True))
            if s <= nb:
                go(ow_hop(s, half, False))

    def ow_wait(s):
        for half in range(2):
            if s <= nf:
                ow_hop(s, half, True, True).wait_recv()
            if s <= nb:
                ow_hop(s, half, False, True).wait_recv()

    def ow_share(n, half):
        place = (z, y)[half]
        slot = lax.rem(place + (nz - (n + 1) // 2 if n % 2 else n // 2), nz)
        src, dst = (wt.at[0, slot], pwt.at[0, slot]) if half == 0 else (wt.at[1, :, slot], pwt.at[1, :, slot])
        return rcopy(src, dst, pw_ss.at[n, half], pw_rs.at[n, half], partner)

    def ow_pass(s):
        if nc > 1:
            for n in (2 * s - 1, 2 * s) if s else (0,):
                if n < nz:
                    for half in range(2):
                        ow_share(n, half).start()

    ow_start(1)
    ow_pass(0)
    kv_advance(1)
    scores = dot_nt(rq, rk) * fade
    inner = dot(scores.astype(BF), rv)
    reaching = rq.astype(F32) * reach

    kv_advance(2)

    for d in range(1, ny):
        p, dev = y_peer(ny - d)
        rcopy(sa.at[p], ra.at[p], a_ss.at[d, 0], a_rs.at[d, 0], dev).wait_recv()
        rcopy(sda, rda.at[p], a_ss.at[d, 1], a_rs.at[d, 1], dev).wait_recv()
    total = ra[0]
    decay = rda[0]
    for i in range(1, ny):
        total = rda[i] * total + ra[i]
        decay = decay * rda[i]
    sb[...] = total
    sdb[...] = decay
    rb[pl.ds(z, 1)] = jnp.zeros((1, sl, BLK), F32)
    rdb[pl.ds(z, 1)] = jnp.zeros((1, 1, BLK), F32)
    for d in range(1, nz):
        dev = z_peer(d)[1]
        go(rcopy(sb, rb.at[z], b_ss.at[d, 0], b_rs.at[d, 0], dev))
        go(rcopy(sdb, rdb.at[z], b_ss.at[d, 1], b_rs.at[d, 1], dev))

    ow_wait(1)
    if nf > 1:
        ow_start(2)
    ow_pass(1)
    for d in range(1, ny):
        rcopy(qbuf.at[0], qbuf.at[d], q_ss.at[d], q_rs.at[d], b_peer(ny - d)).wait_recv()

    krow, lane = iota((BLK, 2 * BLK), 0), iota((BLK, 2 * BLK), 1)
    qlane = jnp.where(lane >= BLK, lane - BLK, lane)
    steps = [0] + [(nz - (s + 1) // 2 if s % 2 else s // 2) for s in range(1, nz)]
    places = [a_place(lax.rem(a + step, nz)) for step in steps]
    key_blocks = [kz * ny + ky for kz, ky in places]
    top_half = row < 64

    def pair(i):
        return nz // 2 - i, lax.rem(nz // 2 + 1 + i, nz)

    def attend(i, lo, hi):
        places, wide = [], []
        for d in pair(i):
            places.append(b_place(lax.rem(b - d + nz, nz)))
            q = qbuf[d]
            zero = jnp.zeros_like(q)
            wide += [jnp.where(top_half, q, zero), jnp.where(top_half, zero, q)]
        blocks = [qz * ny + qy for qz, qy in places]
        s_all = dot(kall[lo * BLK : hi * BLK, :], jnp.concatenate(wide, axis=1))
        probs, peaks, totals = [], [], []
        for n in range(2):
            pieces = []
            for m in range(lo, hi):
                s = s_all[(m - lo) * BLK : (m - lo + 1) * BLK, n * 256 : (n + 1) * 256]
                if m == 0:
                    s = jnp.where(krow + key_blocks[0] * BLK <= qlane + blocks[n] * BLK, s, -HUGE)
                else:
                    s = s + jnp.where(key_blocks[m] < blocks[n], 0.0, -HUGE)
                pieces.append(s)
            s = jnp.concatenate(pieces, axis=0)
            peak = jnp.max(s, axis=0, keepdims=True)
            if lo == 0:
                peak = jnp.maximum(peak, FLOOR)
            else:
                peak = jnp.maximum(peak, early_stat[i, 0:1, n * 256 : (n + 1) * 256])
            p = jnp.exp(s - peak)
            peaks.append(peak)
            totals.append(jnp.sum(p, axis=0, keepdims=True))
            probs.append(p.astype(BF))
        sums = dot(vtall[:, lo * BLK : hi * BLK], jnp.concatenate(probs, axis=1))
        return sums, jnp.concatenate(peaks, axis=1), jnp.concatenate(totals, axis=1), places

    def attend_early(i, _):
        sums, peak, total, _ = attend(i, 0, early)
        early_sum[pl.ds(i, 1)] = sums[None]
        early_stat[pl.ds(i, 1)] = jnp.concatenate([peak, total], axis=0)[None]
        return 0

    def attend_late(i, _):
        first, second = pair(i)
        sums, peak, total, places = attend(i, early, nz)
        share = jnp.exp(early_stat[i, 0:1, :] - peak)
        total = total + share * early_stat[i, 1:2, :]
        sums = (sums + share * early_sum[i]).astype(BF)
        stat = jnp.concatenate([peak, total], axis=0)
        so[pl.ds(first, 1)] = sums[None, :, 0:256]
        so[pl.ds(second, 1)] = sums[None, :, 256:512]
        st[pl.ds(first, 1)] = stat[None, :, 0:256]
        st[pl.ds(second, 1)] = stat[None, :, 256:512]

        def send(d, place):
            dev = (*place, fx, c)
            rcopy(so.at[d], ro.at[d], r_ss.at[d, 0], r_rs.at[d, 0], dev).start()
            rcopy(st.at[d], rst.at[d], r_ss.at[d, 1], r_rs.at[d, 1], dev).start()

        send(first, places[0])

        @pl.when(i < nz // 2 - 1)
        def _():
            send(second, places[1])

        return 0

    lax.fori_loop(0, nz // 4, attend_early, 0)
    if nf > 2:
        kv_advance(3)
    lax.fori_loop(nz // 4, nz // 2, attend_early, 0)
    for s in range(4, nf + 1):
        kv_advance(s)

    for d in range(1, nz):
        p, dev = z_peer(nz - d)
        rcopy(sb, rb.at[p], b_ss.at[d, 0], b_rs.at[d, 0], dev).wait_recv()
        rcopy(sdb, rdb.at[p], b_ss.at[d, 1], b_rs.at[d, 1], dev).wait_recv()
    entry = init[0, pl.ds(pl.multiple_of(y * sl, sl), sl), :].astype(F32)
    for i in range(nz):
        entry = jnp.where(i < z, rdb[i] * entry + rb[i], entry)
    for i in range(ny):
        sc[i] = entry
        entry = rda[i] * entry + ra[i]
    rc[pl.ds(y, 1)] = sc[pl.ds(y, 1)]
    for d in range(1, ny):
        p, dev = y_peer(d)
        rcopy(sc.at[p], rc.at[y], c_ss.at[d], c_rs.at[d], dev).start()

    if nf > 2:
        ow_wait(2)
        ow_start(3)
        ow_pass(2)
    lax.fori_loop(0, nz // 2, attend_late, 0)
    for s in range(3, nf):
        ow_wait(s)
        ow_start(s + 1)
        ow_pass(s)


    width = out_ref.shape[1]
    ow_wait(nf)
    ow_pass(nf)
    for half in range(2):
        wpair[half * BLK : (half + 1) * BLK, :] = wt[half].reshape(width, BLK).astype(F32).T.astype(BF)
    if nc > 1:
        for n in range(nz):
            for half in range(2):
                ow_share(n, half).wait_recv()
        for half in range(2):
            wpair[(2 + half) * BLK : (3 + half) * BLK, :] = pwt[half].reshape(width, BLK).astype(F32).T.astype(BF)

    for d in range(1, ny):
        p, dev = y_peer(ny - d)
        rcopy(sc.at[p], rc.at[p], c_ss.at[d], c_rs.at[d], dev).wait_recv()
    ret = inner + dot(reaching, rc[...].reshape(BLK, BLK), precision=HIGH)
    centre = ret - jnp.mean(ret, axis=-1, keepdims=True)
    ret_mix = (
        centre * lax.rsqrt(jnp.mean(centre * centre, axis=-1, keepdims=True) + EPS) * rgain[...]
    ).astype(BF)

    for d in range(1, ny):
        rcopy(so.at[d], ro.at[d], r_ss.at[d, 0], r_rs.at[d, 0], b_peer(d)).wait_recv()
        rcopy(st.at[d], rst.at[d], r_ss.at[d, 1], r_rs.at[d, 1], b_peer(d)).wait_recv()
    stats = [st[0]] + [rst[d] for d in range(1, ny)]
    top = stats[0][0:1]
    for one in stats[1:]:
        top = jnp.maximum(top, one[0:1])
    total = jnp.zeros_like(top)
    merged = jnp.zeros((BLK, 2 * BLK), F32)
    for d in range(ny):
        share = jnp.exp(stats[d][0:1] - top)
        total = total + share * stats[d][1:2]
        merged = merged + (so[0] if d == 0 else ro[d]).astype(F32) * share
    merged = merged / total
    diff = merged[:, 0:128] - lam_s[0] * merged[:, 128:256]
    diff = diff * lax.rsqrt(jnp.mean(diff * diff, axis=0, keepdims=True) + EPS)
    diff_mix = (diff.T * dgain[...]).astype(BF)

    mix = jnp.concatenate([ret_mix, diff_mix], axis=1)
    mixb[...] = mix.reshape(nx, nc, rows, 256)
    if nc > 1:
        swap = rcopy(mixb.at[:, 1 - c], pmix, mix_ss, mix_rs, partner)
        go(swap)
        swap.wait_recv()
        mine = mixb[:, pl.ds(c, 1)].reshape(nx * rows, 256)
        mix = jnp.concatenate([mine, pmix[...].reshape(nx * rows, 256)], axis=1)
    fs[...] = dot(mix, wpair[...]).astype(BF).reshape(nx, rows, width)
    for d in range(1, nx):
        p, dev = x_peer(d)
        go(rcopy(fs.at[p], fr.at[d], f_ss.at[d], f_rs.at[d], dev))
    acc = fs[pl.ds(fx, 1)].reshape(rows, width).astype(F32)
    for d in range(1, nx):
        rcopy(fs.at[0], fr.at[d], f_ss.at[d], f_rs.at[d], x_peer(d)[1]).wait_recv()
        acc = acc + fr[d].astype(F32)
    out_ref[...] = acc.astype(BF)

    for copy in sends:
        copy.wait_send()
    if nc > 1:
        for n in range(nz):
            for half in range(2):
                ow_share(n, half).wait_send()
    for d in range(1, ny):
        p, dev = y_peer(d)
        rcopy(sc.at[p], rc.at[y], c_ss.at[d], c_rs.at[d], dev).wait_send()
        rcopy(so.at[d], ro.at[d], r_ss.at[d, 0], r_rs.at[d, 0], b_peer(d)).wait_send()
        rcopy(st.at[d], rst.at[d], r_ss.at[d, 1], r_rs.at[d, 1], b_peer(d)).wait_send()


def local(
    dims, tokens, in_gain, ret_query, ret_key, ret_value, decay_log, init_state, ret_gain,
    diff_query, diff_key, diff_value, diff_lambda, diff_gain, out_weight,
):
    nz, ny, nx, nc = dims
    nh = nx * nc
    rows, width = tokens.shape
    sl = BLK // ny
    nf, nb = nz // 2, nz - 1 - nz // 2
    dma = pltpu.SemaphoreType.DMA
    vm = pltpu.VMEM
    scratch = [
        vm((rows, width), BF), vm((1, width), F32), vm((1, BLK), F32), vm((1, BLK, BLK), BF),
        vm((1, BLK), F32), vm((1, BLK), F32), vm((2, BLK, width), BF), vm((width, 768), BF), vm((BLK, width), BF),
        vm((nz * BLK, BLK), BF), vm((BLK, nz * BLK), BF), vm((ny, BLK, BLK), BF),
        vm((ny, BLK, 2 * BLK), BF), vm((ny, 2, 2 * BLK), F32), vm((ny, BLK, 2 * BLK), BF), vm((ny, 2, 2 * BLK), F32),
        vm((ny, sl, BLK), F32), vm((1, BLK), F32), vm((ny, sl, BLK), F32), vm((ny, 1, BLK), F32),
        vm((sl, BLK), F32), vm((1, BLK), F32), vm((nz, sl, BLK), F32), vm((nz, 1, BLK), F32),
        vm((ny, sl, BLK), F32), vm((ny, sl, BLK), F32),
        vm((nz // 2, BLK, 4 * BLK), F32), vm((nz // 2, 2, 4 * BLK), F32),
        vm((2, nz, ny, 32, BLK), BF), vm((2, nz, ny, 32, BLK), BF), vm((2 * nc * BLK, width), BF),
        vm((nx, nc, rows, 2 * BLK), BF), vm((nx, rows, 2 * BLK), BF), vm((nx, rows, width), BF), vm((nx, rows, width), BF),
        dma((13,)), dma((nx,)), dma((nx,)), dma((nx,)), dma((nx,)), dma((ny, 2)), dma((ny, 2)),
        dma((nf, 2)), dma((nf, 2)), dma((max(nb, 1), 2)), dma((max(nb, 1), 2)), dma((ny,)), dma((ny,)),
        dma((ny, 2)), dma((ny, 2)), dma((nz, 2)), dma((nz, 2)), dma((ny,)), dma((ny,)),
        dma((ny, 2)), dma((ny, 2)), dma((nf, 2)), dma((nf, 2)), dma((max(nb, 1), 2)), dma((max(nb, 1), 2)),
        dma((nz, 2)), dma((nz, 2)), dma, dma, dma((nx,)), dma((nx,)),
    ]
    anyspec = pl.BlockSpec(memory_space=pl.ANY)
    smem = pl.BlockSpec(memory_space=pltpu.SMEM)
    return pl.pallas_call(
        functools.partial(kernel, dims),
        out_shape=jax.ShapeDtypeStruct((rows, width), BF),
        in_specs=[anyspec] * 11 + [smem] + [anyspec] * 2,
        out_specs=pl.BlockSpec(memory_space=pltpu.VMEM),
        scratch_shapes=scratch,
        compiler_params=pltpu.CompilerParams(
            collective_id=0, has_side_effects=True, vmem_limit_bytes=60 * 1024 * 1024
        ),
    )(
        tokens,
        in_gain.reshape(1, width),
        ret_query,
        ret_key,
        ret_value,
        decay_log,
        init_state,
        ret_gain.reshape(1, BLK),
        jnp.swapaxes(diff_query, 1, 2).reshape(BLK, width),
        jnp.swapaxes(diff_key, 1, 2).reshape(BLK, width),
        diff_value,
        diff_lambda,
        diff_gain.reshape(1, BLK),
        jnp.swapaxes(out_weight, 1, 2),
    )


def build(split):
    dims = tuple(split.shape[a] for a in SP_FS_TP)
    placed = (
        P(SP_FS_TP, None),
        P(),
        P(None, ("fs", "tp")),
        P(None, ("fs", "tp")),
        P(None, ("fs", "tp")),
        P(("fs", "tp"), SP),
        P(("fs", "tp"), None, None),
        P(("fs", "tp")),
        P(None, None, ("fs", "tp")),
        P(None, None, ("fs", "tp")),
        P(None, ("fs", "tp")),
        P(("fs", "tp")),
        P(("fs", "tp")),
        P(None, ("fs", "tp"), SP),
    )
    return jax.shard_map(
        functools.partial(local, dims), mesh=split, in_specs=placed, out_specs=P(SP_FS_TP, None), check_vma=False
    )


def solution(mesh):
    return build(Mesh(mesh.devices.reshape(8, 8, mesh.shape["fs"], mesh.shape["tp"]), SP_FS_TP))
```

```python
import functools

import jax
import jax.numpy as jnp
from jax import lax
from jax.experimental import pallas as pl
from jax.experimental.pallas import tpu as pltpu
from jax.sharding import Mesh
from jax.sharding import PartitionSpec as P

SP = ("sp_0", "sp_1")
SP_FS_TP = ("sp_0", "sp_1", "fs", "tp")
MESH = pl.DeviceIdType.MESH
EPS = 1e-06
HUGE = 1e30
FLOOR = -1e29
BLK = 128
BF = jnp.bfloat16
F32 = jnp.float32
HIGH = lax.Precision.HIGHEST


def dot(a, b, **kw):
    return jnp.dot(a, b, preferred_element_type=F32, **kw)


def dot_nt(a, b):
    return lax.dot_general(a, b, (((1,), (1,)), ((), ())), preferred_element_type=F32)


def iota(shape, dim):
    return lax.broadcasted_iota(jnp.int32, shape, dim)


def kernel(
    dims,
    tok_h, gain_h, wrq_h, wrk_h, wrv_h, dec_h, init_h, rgain_h, wq_h, wk_h, wv_h, lam_s, dgain_h, ow_h,
    out_ref,
    tok, gain, dec, init, rgain, dgain, wqk, w, x,
    kall, vtall, qbuf, so, st, ro, rst,
    sa, sda, ra, rda, sb, sdb, rb, rdb, sc, rc,
    early_sum, early_stat, wt, pwt, wpair, mixb, pmix, fs, fr,
    in_sem, tok_ss, tok_rs, pt_ss, pt_rs, ow_ss, ow_rs, kf_ss, kf_rs, kb_ss, kb_rs, q_ss, q_rs,
    a_ss, a_rs, b_ss, b_rs, c_ss, c_rs, r_ss, r_rs, wf_ss, wf_rs, wb_ss, wb_rs, pw_ss, pw_rs, mix_ss, mix_rs, f_ss, f_rs,
):
    nz, ny, nx, nc = dims
    nh = nx * nc
    rows = BLK // nh
    sl = BLK // ny
    nf, nb = nz // 2, nz - 1 - nz // 2
    early = 5 if nz > 5 else 3
    z, y = lax.axis_index("sp_0"), lax.axis_index("sp_1")
    fx, c = lax.axis_index("fs"), lax.axis_index("tp")
    h = fx * nc + c

    def head_peer(d):
        p = lax.rem(h + d, nh)
        return p, (z, y, p // nc, lax.rem(p, nc))

    a, b = (1 - c) * z + c * y, (1 - c) * y + c * z

    def a_place(p):
        return z + (1 - c) * (p - a), y + c * (p - a)

    def b_place(p):
        return z + c * (p - b), y + (1 - c) * (p - b)

    def a_peer(d):
        return (*a_place(lax.rem(a + d, nz)), fx, c)

    def b_peer(d):
        return (*b_place(lax.rem(b + d, nz)), fx, c)

    def x_peer(d):
        p = lax.rem(fx + d, nx)
        return p, (z, y, p, c)

    partner = (z, y, fx, 1 - c)

    def y_peer(d):
        p = lax.rem(y + d, ny)
        return p, (z, p, fx, c)

    def z_peer(d):
        p = lax.rem(z + d, nz)
        return p, (p, y, fx, c)

    def rcopy(src, dst, ss, rs, dev):
        return pltpu.make_async_remote_copy(
            src_ref=src, dst_ref=dst, send_sem=ss, recv_sem=rs, device_id=dev, device_id_type=MESH
        )

    barrier = pltpu.get_barrier_semaphore()
    for d in range(1, nh):
        pl.semaphore_signal(barrier, inc=1, device_id=head_peer(d)[1], device_id_type=MESH)
    for d in range(1, ny):
        pl.semaphore_signal(barrier, inc=1, device_id=y_peer(d)[1], device_id_type=MESH)
    for d in range(1, nz):
        pl.semaphore_signal(barrier, inc=1, device_id=z_peer(d)[1], device_id_type=MESH)

    inputs = [
        (tok_h, tok), (gain_h, gain), (ow_h, wt.at[:, z, y]), (wk_h, wqk.at[0]), (wq_h, wqk.at[1]),
        (wv_h, w.at[:, pl.ds(128, 128)]), (wrq_h, w.at[:, pl.ds(384, 128)]),
        (wrk_h, w.at[:, pl.ds(512, 128)]), (wrv_h, w.at[:, pl.ds(640, 128)]),
        (dec_h, dec), (init_h, init), (rgain_h, rgain), (dgain_h, dgain),
    ]
    loads = [pltpu.make_async_copy(s, t, in_sem.at[i]) for i, (s, t) in enumerate(inputs)]
    for copy in loads:
        copy.start()

    loads[0].wait()
    loads[1].wait()
    t = tok[...].astype(F32)
    scale = lax.rsqrt(jnp.mean(t * t, axis=-1, keepdims=True) + EPS)
    own_x = x.at[pl.ds(pl.multiple_of(h * rows, rows), rows), :]
    own_x[...] = (t * scale * gain[...]).astype(BF)
    loads[2].wait()

    pl.semaphore_wait(barrier, nh + ny + nz - 3)

    sends = []

    def go(copy):
        copy.start()
        sends.append(copy)

    def x_rows(p, core):
        return x.at[pl.ds(pl.multiple_of((p * nc + core) * rows, rows), rows), :]

    for d in range(1, nx):
        go(rcopy(own_x, own_x, tok_ss.at[d], tok_rs.at[d], x_peer(d)[1]))
    if nc > 1:
        go(rcopy(own_x, own_x, pt_ss.at[0], pt_rs.at[0], partner))
    for d in range(1, ny):
        part = wt.at[0, z, y]
        go(rcopy(part, part, ow_ss.at[d, 0], ow_rs.at[d, 0], y_peer(d)[1]))
        part = wt.at[1, z, y]
        go(rcopy(part, part, ow_ss.at[d, 1], ow_rs.at[d, 1], z_peer(d)[1]))

    loads[3].wait()
    w[:, 0:128] = wqk[0].astype(F32).T.astype(BF)
    loads[4].wait()
    w[:, 256:384] = wqk[1].astype(F32).T.astype(BF)
    for copy in loads[5:]:
        copy.wait()

    row, col = iota((BLK, BLK), 0), iota((BLK, BLK), 1)
    lower = row >= col
    decb = jnp.broadcast_to(dec[...], (BLK, BLK))
    cum_col = jnp.sum(jnp.where(lower, decb, 0.0), axis=1, keepdims=True)
    dec_col = jnp.sum(jnp.where(row == col, decb, 0.0), axis=1, keepdims=True)
    cum_row = jnp.sum(jnp.where(row <= col, jnp.broadcast_to(dec_col, (BLK, BLK)), 0.0), axis=0, keepdims=True)
    cum_end = jnp.sum(dec[...], axis=1, keepdims=True)
    fade = jnp.exp(jnp.where(lower, cum_col - cum_row, -HUGE)) * (BLK ** (-0.5))
    key_weight = jnp.exp(cum_end - cum_col) * (BLK ** (-0.5))
    reach = jnp.exp(cum_col)
    sda[...] = jnp.broadcast_to(jnp.exp(cum_end), sda.shape)

    for d in sorted(range(1, nx), key=lambda v: min(v, nx - v)):
        p, dev = x_peer(nx - d)
        part = x_rows(p, c)
        rcopy(part, part, tok_ss.at[d], tok_rs.at[d], dev).wait_recv()
        if nc > 1:
            go(rcopy(part, part, pt_ss.at[d], pt_rs.at[d], partner))
    for d in range(1, ny):
        part = wt.at[0, z, y_peer(ny - d)[0]]
        rcopy(part, part, ow_ss.at[d, 0], ow_rs.at[d, 0], partner).wait_recv()
        part = wt.at[1, z_peer(nz - d)[0], y]
        rcopy(part, part, ow_ss.at[d, 1], ow_rs.at[d, 1], partner).wait_recv()

    def ow_hop(s, half, forward, arriving=False):
        place, peer = ((z, z_peer), (y, y_peer))[half]
        back = s if arriving else s - 1
        slot = lax.rem(place + (nz - back if forward else back), nz)
        ref = wt.at[0, slot] if half == 0 else wt.at[1, :, slot]
        ss, rs = (wf_ss, wf_rs) if forward else (wb_ss, wb_rs)
        return rcopy(ref, ref, ss.at[s - 1, half], rs.at[s - 1, half], peer(1 if forward else nz - 1)[1])

    def ow_start(s):
        for half in range(2):
            if s <= nf:
                go(ow_hop(s, half, True))
            if s <= nb:
                go(ow_hop(s, half, False))

    def ow_wait(s):
        for half in range(2):
            if s <= nf:
                ow_hop(s, half, True, True).wait_recv()
            if s <= nb:
                ow_hop(s, half, False, True).wait_recv()

    def ow_share(n, half):
        place = (z, y)[half]
        slot = lax.rem(place + (nz - (n + 1) // 2 if n % 2 else n // 2), nz)
        src, dst = (wt.at[0, slot], pwt.at[0, slot]) if half == 0 else (wt.at[1, :, slot], pwt.at[1, :, slot])
        return rcopy(src, dst, pw_ss.at[n, half], pw_rs.at[n, half], partner)

    def ow_pass(s):
        if nc > 1:
            for n in (2 * s - 1, 2 * s) if s else (0,):
                if n < nz:
                    for half in range(2):
                        ow_share(n, half).start()

    ow_start(1)
    ow_pass(0)

    if nc > 1:
        for d in range(nx):
            part = x_rows(lax.rem(fx + nx - d, nx), 1 - c)
            rcopy(part, part, pt_ss.at[d], pt_rs.at[d], partner).wait_recv()

    xs = x[...]
    kv = dot(xs, w[:, 0:256])
    kall[0:BLK, :] = kv[:, 0:128].astype(BF)
    vtall[:, 0:BLK] = kv[:, 128:256].T.astype(BF)

    def k_at(s):
        return kall.at[pl.ds(s * BLK, BLK), :]

    def v_at(s):
        return vtall.at[:, pl.ds(s * BLK, BLK)]

    right, left = a_peer(1), a_peer(nz - 1)

    def kv_hop(s, forward, part):
        if part == 2:
            src, dst = (s - 1, s) if forward else ((nz - s + 1) % nz, nz - s)
            return rcopy(qbuf.at[src], qbuf.at[dst], q_ss.at[dst], q_rs.at[dst], b_peer(1 if forward else nz - 1))
        if forward:
            src, dst, ss, rs, dev = max(2 * s - 3, 0), 2 * s - 1, kf_ss, kf_rs, right
        else:
            src, dst, ss, rs, dev = 2 * s - 2, 2 * s, kb_ss, kb_rs, left
        at = (k_at, v_at)[part]
        return rcopy(at(src), at(dst), ss.at[s - 1, part], rs.at[s - 1, part], dev)

    def kv_start(s, parts):
        for part in parts:
            if s <= nf:
                go(kv_hop(s, True, part))
            if s <= nb:
                go(kv_hop(s, False, part))

    def kv_advance(s):
        for part in range(3):
            if s <= nf:
                kv_hop(s, True, part).wait_recv()
                if s + 1 <= nf:
                    go(kv_hop(s + 1, True, part))
            if s <= nb:
                kv_hop(s, False, part).wait_recv()
                if s + 1 <= nb:
                    go(kv_hop(s + 1, False, part))

    kv_start(1, (0, 1))

    rest = dot(xs, w[:, 256:768])
    qbuf[0] = (rest[:, 0:128].astype(BF).astype(F32) * (64 ** (-0.5))).T.astype(BF)
    kv_start(1, (2,))

    rq, rk, rv = (rest[:, 128 * i : 128 * (i + 1)].astype(BF) for i in (1, 2, 3))
    keyed = (rk.astype(F32) * key_weight).T
    state = dot(keyed, rv.astype(F32), precision=HIGH)
    sa[...] = state.reshape(ny, sl, BLK)
    ra[pl.ds(y, 1)] = sa[pl.ds(y, 1)]
    rda[pl.ds(y, 1)] = sda[...].reshape(1, 1, BLK)
    for d in range(1, ny):
        p, dev = y_peer(d)
        go(rcopy(sa.at[p], ra.at[y], a_ss.at[d, 0], a_rs.at[d, 0], dev))
        go(rcopy(sda, rda.at[y], a_ss.at[d, 1], a_rs.at[d, 1], dev))

    kv_advance(1)
    scores = dot_nt(rq, rk) * fade
    inner = dot(scores.astype(BF), rv)
    reaching = rq.astype(F32) * reach

    ow_wait(1)
    ow_start(2)
    ow_pass(1)
    kv_advance(2)

    for d in range(1, ny):
        p, dev = y_peer(ny - d)
        rcopy(sa.at[p], ra.at[p], a_ss.at[d, 0], a_rs.at[d, 0], dev).wait_recv()
        rcopy(sda, rda.at[p], a_ss.at[d, 1], a_rs.at[d, 1], dev).wait_recv()
    total = ra[0]
    decay = rda[0]
    for i in range(1, ny):
        total = rda[i] * total + ra[i]
        decay = decay * rda[i]
    sb[...] = total
    sdb[...] = decay
    rb[pl.ds(z, 1)] = jnp.zeros((1, sl, BLK), F32)
    rdb[pl.ds(z, 1)] = jnp.zeros((1, 1, BLK), F32)
    for d in range(1, nz):
        dev = z_peer(d)[1]
        go(rcopy(sb, rb.at[z], b_ss.at[d, 0], b_rs.at[d, 0], dev))
        go(rcopy(sdb, rdb.at[z], b_ss.at[d, 1], b_rs.at[d, 1], dev))

    krow, lane = iota((BLK, 2 * BLK), 0), iota((BLK, 2 * BLK), 1)
    qlane = jnp.where(lane >= BLK, lane - BLK, lane)
    steps = [0] + [(nz - (s + 1) // 2 if s % 2 else s // 2) for s in range(1, nz)]
    places = [a_place(lax.rem(a + step, nz)) for step in steps]
    key_blocks = [kz * ny + ky for kz, ky in places]
    top_half = row < 64

    def pair(i):
        return nz // 2 - i, lax.rem(nz // 2 + 1 + i, nz)

    def attend(i, lo, hi):
        places, wide = [], []
        for d in pair(i):
            places.append(b_place(lax.rem(b - d + nz, nz)))
            q = qbuf[d]
            zero = jnp.zeros_like(q)
            wide += [jnp.where(top_half, q, zero), jnp.where(top_half, zero, q)]
        blocks = [qz * ny + qy for qz, qy in places]
        s_all = dot(kall[lo * BLK : hi * BLK, :], jnp.concatenate(wide, axis=1))
        probs, peaks, totals = [], [], []
        for n in range(2):
            pieces = []
            for m in range(lo, hi):
                s = s_all[(m - lo) * BLK : (m - lo + 1) * BLK, n * 256 : (n + 1) * 256]
                if m == 0:
                    s = jnp.where(krow + key_blocks[0] * BLK <= qlane + blocks[n] * BLK, s, -HUGE)
                else:
                    s = s + jnp.where(key_blocks[m] < blocks[n], 0.0, -HUGE)
                pieces.append(s)
            s = jnp.concatenate(pieces, axis=0)
            peak = jnp.max(s, axis=0, keepdims=True)
            if lo == 0:
                peak = jnp.maximum(peak, FLOOR)
            else:
                peak = jnp.maximum(peak, early_stat[i, 0:1, n * 256 : (n + 1) * 256])
            p = jnp.exp(s - peak)
            peaks.append(peak)
            totals.append(jnp.sum(p, axis=0, keepdims=True))
            probs.append(p.astype(BF))
        sums = dot(vtall[:, lo * BLK : hi * BLK], jnp.concatenate(probs, axis=1))
        return sums, jnp.concatenate(peaks, axis=1), jnp.concatenate(totals, axis=1), places

    def attend_early(near, _):
        i = nz // 2 - 1 - near
        sums, peak, total, _ = attend(i, 0, early)
        early_sum[pl.ds(i, 1)] = sums[None]
        early_stat[pl.ds(i, 1)] = jnp.concatenate([peak, total], axis=0)[None]
        return 0

    def attend_late(i, _):
        first, second = pair(i)
        sums, peak, total, places = attend(i, early, nz)
        share = jnp.exp(early_stat[i, 0:1, :] - peak)
        total = total + share * early_stat[i, 1:2, :]
        sums = (sums + share * early_sum[i]).astype(BF)
        stat = jnp.concatenate([peak, total], axis=0)
        so[pl.ds(first, 1)] = sums[None, :, 0:256]
        so[pl.ds(second, 1)] = sums[None, :, 256:512]
        st[pl.ds(first, 1)] = stat[None, :, 0:256]
        st[pl.ds(second, 1)] = stat[None, :, 256:512]

        def send(d, place):
            dev = (*place, fx, c)
            rcopy(so.at[d], ro.at[d], r_ss.at[d, 0], r_rs.at[d, 0], dev).start()
            rcopy(st.at[d], rst.at[d], r_ss.at[d, 1], r_rs.at[d, 1], dev).start()

        send(first, places[0])

        @pl.when(i < nz // 2 - 1)
        def _():
            send(second, places[1])

        return 0

    pairs = nz // 2
    lax.fori_loop(0, min(2, pairs), attend_early, 0)
    for s in range(3, nf + 1):
        ow_wait(s - 1)
        ow_start(s)
        ow_pass(s - 1)
        kv_advance(s)
        lax.fori_loop(s - 1, s, attend_early, 0)

    for d in range(1, nz):
        p, dev = z_peer(nz - d)
        rcopy(sb, rb.at[p], b_ss.at[d, 0], b_rs.at[d, 0], dev).wait_recv()
        rcopy(sdb, rdb.at[p], b_ss.at[d, 1], b_rs.at[d, 1], dev).wait_recv()
    entry = init[0, pl.ds(pl.multiple_of(y * sl, sl), sl), :].astype(F32)
    for i in range(nz):
        entry = jnp.where(i < z, rdb[i] * entry + rb[i], entry)
    for i in range(ny):
        sc[i] = entry
        entry = rda[i] * entry + ra[i]
    rc[pl.ds(y, 1)] = sc[pl.ds(y, 1)]
    for d in range(1, ny):
        p, dev = y_peer(d)
        rcopy(sc.at[p], rc.at[y], c_ss.at[d], c_rs.at[d], dev).start()

    lax.fori_loop(0, pairs, attend_late, 0)

    width = out_ref.shape[1]
    ow_wait(nf)
    ow_pass(nf)
    for half in range(2):
        wpair[half * BLK : (half + 1) * BLK, :] = wt[half].reshape(width, BLK).astype(F32).T.astype(BF)
    if nc > 1:
        for n in range(nz):
            for half in range(2):
                ow_share(n, half).wait_recv()
        for half in range(2):
            wpair[(2 + half) * BLK : (3 + half) * BLK, :] = pwt[half].reshape(width, BLK).astype(F32).T.astype(BF)

    for d in range(1, ny):
        p, dev = y_peer(ny - d)
        rcopy(sc.at[p], rc.at[p], c_ss.at[d], c_rs.at[d], dev).wait_recv()
    ret = inner + dot(reaching, rc[...].reshape(BLK, BLK), precision=HIGH)
    centre = ret - jnp.mean(ret, axis=-1, keepdims=True)
    ret_mix = (
        centre * lax.rsqrt(jnp.mean(centre * centre, axis=-1, keepdims=True) + EPS) * rgain[...]
    ).astype(BF)

    for d in range(1, ny):
        rcopy(so.at[d], ro.at[d], r_ss.at[d, 0], r_rs.at[d, 0], b_peer(d)).wait_recv()
        rcopy(st.at[d], rst.at[d], r_ss.at[d, 1], r_rs.at[d, 1], b_peer(d)).wait_recv()
    stats = [st[0]] + [rst[d] for d in range(1, ny)]
    top = stats[0][0:1]
    for one in stats[1:]:
        top = jnp.maximum(top, one[0:1])
    total = jnp.zeros_like(top)
    merged = jnp.zeros((BLK, 2 * BLK), F32)
    for d in range(ny):
        share = jnp.exp(stats[d][0:1] - top)
        total = total + share * stats[d][1:2]
        merged = merged + (so[0] if d == 0 else ro[d]).astype(F32) * share
    merged = merged / total
    diff = merged[:, 0:128] - lam_s[0] * merged[:, 128:256]
    diff = diff * lax.rsqrt(jnp.mean(diff * diff, axis=0, keepdims=True) + EPS)
    diff_mix = (diff.T * dgain[...]).astype(BF)

    mix = jnp.concatenate([ret_mix, diff_mix], axis=1)
    mixb[...] = mix.reshape(nx, nc, rows, 256)
    if nc > 1:
        swap = rcopy(mixb.at[:, 1 - c], pmix, mix_ss, mix_rs, partner)
        go(swap)
        swap.wait_recv()
        mine = mixb[:, pl.ds(c, 1)].reshape(nx * rows, 256)
        mix = jnp.concatenate([mine, pmix[...].reshape(nx * rows, 256)], axis=1)
    fs[...] = dot(mix, wpair[...]).astype(BF).reshape(nx, rows, width)
    for d in range(1, nx):
        p, dev = x_peer(d)
        go(rcopy(fs.at[p], fr.at[d], f_ss.at[d], f_rs.at[d], dev))
    acc = fs[pl.ds(fx, 1)].reshape(rows, width).astype(F32)
    for d in range(1, nx):
        rcopy(fs.at[0], fr.at[d], f_ss.at[d], f_rs.at[d], x_peer(d)[1]).wait_recv()
        acc = acc + fr[d].astype(F32)
    out_ref[...] = acc.astype(BF)

    for copy in sends:
        copy.wait_send()
    if nc > 1:
        for n in range(nz):
            for half in range(2):
                ow_share(n, half).wait_send()
    for d in range(1, ny):
        p, dev = y_peer(d)
        rcopy(sc.at[p], rc.at[y], c_ss.at[d], c_rs.at[d], dev).wait_send()
        rcopy(so.at[d], ro.at[d], r_ss.at[d, 0], r_rs.at[d, 0], b_peer(d)).wait_send()
        rcopy(st.at[d], rst.at[d], r_ss.at[d, 1], r_rs.at[d, 1], b_peer(d)).wait_send()


def local(
    dims, tokens, in_gain, ret_query, ret_key, ret_value, decay_log, init_state, ret_gain,
    diff_query, diff_key, diff_value, diff_lambda, diff_gain, out_weight,
):
    nz, ny, nx, nc = dims
    nh = nx * nc
    rows, width = tokens.shape
    sl = BLK // ny
    nf, nb = nz // 2, nz - 1 - nz // 2
    dma = pltpu.SemaphoreType.DMA
    vm = pltpu.VMEM
    scratch = [
        vm((rows, width), BF), vm((1, width), F32), vm((1, BLK), F32), vm((1, BLK, BLK), BF),
        vm((1, BLK), F32), vm((1, BLK), F32), vm((2, BLK, width), BF), vm((width, 768), BF), vm((BLK, width), BF),
        vm((nz * BLK, BLK), BF), vm((BLK, nz * BLK), BF), vm((ny, BLK, BLK), BF),
        vm((ny, BLK, 2 * BLK), BF), vm((ny, 2, 2 * BLK), F32), vm((ny, BLK, 2 * BLK), BF), vm((ny, 2, 2 * BLK), F32),
        vm((ny, sl, BLK), F32), vm((1, BLK), F32), vm((ny, sl, BLK), F32), vm((ny, 1, BLK), F32),
        vm((sl, BLK), F32), vm((1, BLK), F32), vm((nz, sl, BLK), F32), vm((nz, 1, BLK), F32),
        vm((ny, sl, BLK), F32), vm((ny, sl, BLK), F32),
        vm((nz // 2, BLK, 4 * BLK), F32), vm((nz // 2, 2, 4 * BLK), F32),
        vm((2, nz, ny, 32, BLK), BF), vm((2, nz, ny, 32, BLK), BF), vm((2 * nc * BLK, width), BF),
        vm((nx, nc, rows, 2 * BLK), BF), vm((nx, rows, 2 * BLK), BF), vm((nx, rows, width), BF), vm((nx, rows, width), BF),
        dma((13,)), dma((nx,)), dma((nx,)), dma((nx,)), dma((nx,)), dma((ny, 2)), dma((ny, 2)),
        dma((nf, 2)), dma((nf, 2)), dma((max(nb, 1), 2)), dma((max(nb, 1), 2)), dma((ny,)), dma((ny,)),
        dma((ny, 2)), dma((ny, 2)), dma((nz, 2)), dma((nz, 2)), dma((ny,)), dma((ny,)),
        dma((ny, 2)), dma((ny, 2)), dma((nf, 2)), dma((nf, 2)), dma((max(nb, 1), 2)), dma((max(nb, 1), 2)),
        dma((nz, 2)), dma((nz, 2)), dma, dma, dma((nx,)), dma((nx,)),
    ]
    anyspec = pl.BlockSpec(memory_space=pl.ANY)
    smem = pl.BlockSpec(memory_space=pltpu.SMEM)
    return pl.pallas_call(
        functools.partial(kernel, dims),
        out_shape=jax.ShapeDtypeStruct((rows, width), BF),
        in_specs=[anyspec] * 11 + [smem] + [anyspec] * 2,
        out_specs=pl.BlockSpec(memory_space=pltpu.VMEM),
        scratch_shapes=scratch,
        compiler_params=pltpu.CompilerParams(
            collective_id=0, has_side_effects=True, vmem_limit_bytes=60 * 1024 * 1024
        ),
    )(
        tokens,
        in_gain.reshape(1, width),
        ret_query,
        ret_key,
        ret_value,
        decay_log,
        init_state,
        ret_gain.reshape(1, BLK),
        jnp.swapaxes(diff_query, 1, 2).reshape(BLK, width),
        jnp.swapaxes(diff_key, 1, 2).reshape(BLK, width),
        diff_value,
        diff_lambda,
        diff_gain.reshape(1, BLK),
        jnp.swapaxes(out_weight, 1, 2),
    )


def build(split):
    dims = tuple(split.shape[a] for a in SP_FS_TP)
    placed = (
        P(SP_FS_TP, None),
        P(),
        P(None, ("fs", "tp")),
        P(None, ("fs", "tp")),
        P(None, ("fs", "tp")),
        P(("fs", "tp"), SP),
        P(("fs", "tp"), None, None),
        P(("fs", "tp")),
        P(None, None, ("fs", "tp")),
        P(None, None, ("fs", "tp")),
        P(None, ("fs", "tp")),
        P(("fs", "tp")),
        P(("fs", "tp")),
        P(None, ("fs", "tp"), SP),
    )
    return jax.shard_map(
        functools.partial(local, dims), mesh=split, in_specs=placed, out_specs=P(SP_FS_TP, None), check_vma=False
    )


def solution(mesh):
    return build(Mesh(mesh.devices.reshape(8, 8, mesh.shape["fs"], mesh.shape["tp"]), SP_FS_TP))
```

```python
import functools

import jax
import jax.numpy as jnp
from jax import lax
from jax.experimental import pallas as pl
from jax.experimental.pallas import tpu as pltpu
from jax.sharding import Mesh
from jax.sharding import PartitionSpec as P

SP = ("sp_0", "sp_1")
SP_FS_TP = ("sp_0", "sp_1", "fs", "tp")
MESH = pl.DeviceIdType.MESH
EPS = 1e-06
HUGE = 1e30
FLOOR = -1e29
BLK = 128
RELAY = (None, 0, 1, 2, 3)
BF = jnp.bfloat16
F32 = jnp.float32
HIGH = lax.Precision.HIGHEST


def dot(a, b, **kw):
    return jnp.dot(a, b, preferred_element_type=F32, **kw)


def dot_nt(a, b):
    return lax.dot_general(a, b, (((1,), (1,)), ((), ())), preferred_element_type=F32)


def iota(shape, dim):
    return lax.broadcasted_iota(jnp.int32, shape, dim)


def kernel(
    dims,
    tok_h, gain_h, wrq_h, wrk_h, wrv_h, dec_h, init_h, rgain_h, wq_h, wk_h, wv_h, lam_s, dgain_h, ow_h,
    out_ref,
    tok, gain, dec, init, rgain, dgain, wqk, w, x,
    kall, vtall, qbuf, so, st, ro, rst,
    sa, sda, ra, rda, sb, sdb, rb, rdb, sc, rc,
    early_sum, early_stat, wt, pwt, wpair, mixb, pmix, fs, fr,
    in_sem, tok_ss, tok_rs, pt_ss, pt_rs, ow_ss, ow_rs, kf_ss, kf_rs, kb_ss, kb_rs, q_ss, q_rs,
    a_ss, a_rs, b_ss, b_rs, c_ss, c_rs, r_ss, r_rs, wf_ss, wf_rs, wb_ss, wb_rs, pw_ss, pw_rs, mix_ss, mix_rs, f_ss, f_rs,
):
    nz, ny, nx, nc = dims
    nh = nx * nc
    rows = BLK // nh
    sl = BLK // ny
    nf, nb = nz // 2, nz - 1 - nz // 2
    early = 5 if nz > 5 else 3
    z, y = lax.axis_index("sp_0"), lax.axis_index("sp_1")
    fx, c = lax.axis_index("fs"), lax.axis_index("tp")
    h = fx * nc + c

    def head_peer(d):
        p = lax.rem(h + d, nh)
        return p, (z, y, p // nc, lax.rem(p, nc))

    a, b = (1 - c) * z + c * y, (1 - c) * y + c * z

    def a_place(p):
        return z + (1 - c) * (p - a), y + c * (p - a)

    def b_place(p):
        return z + c * (p - b), y + (1 - c) * (p - b)

    def a_peer(d):
        return (*a_place(lax.rem(a + d, nz)), fx, c)

    def b_peer(d):
        return (*b_place(lax.rem(b + d, nz)), fx, c)

    def x_peer(d):
        p = lax.rem(fx + d, nx)
        return p, (z, y, p, c)

    partner = (z, y, fx, 1 - c)

    def y_peer(d):
        p = lax.rem(y + d, ny)
        return p, (z, p, fx, c)

    def z_peer(d):
        p = lax.rem(z + d, nz)
        return p, (p, y, fx, c)

    def rcopy(src, dst, ss, rs, dev):
        return pltpu.make_async_remote_copy(
            src_ref=src, dst_ref=dst, send_sem=ss, recv_sem=rs, device_id=dev, device_id_type=MESH
        )

    barrier = pltpu.get_barrier_semaphore()
    for d in range(1, nh):
        pl.semaphore_signal(barrier, inc=1, device_id=head_peer(d)[1], device_id_type=MESH)
    for d in range(1, ny):
        pl.semaphore_signal(barrier, inc=1, device_id=y_peer(d)[1], device_id_type=MESH)
    for d in range(1, nz):
        pl.semaphore_signal(barrier, inc=1, device_id=z_peer(d)[1], device_id_type=MESH)

    inputs = [
        (tok_h, tok), (gain_h, gain), (ow_h, wt.at[:, z, y]), (wk_h, wqk.at[0]), (wq_h, wqk.at[1]),
        (wv_h, w.at[:, pl.ds(128, 128)]), (wrq_h, w.at[:, pl.ds(384, 128)]),
        (wrk_h, w.at[:, pl.ds(512, 128)]), (wrv_h, w.at[:, pl.ds(640, 128)]),
        (dec_h, dec), (init_h, init), (rgain_h, rgain), (dgain_h, dgain),
    ]
    loads = [pltpu.make_async_copy(s, t, in_sem.at[i]) for i, (s, t) in enumerate(inputs)]
    for copy in loads:
        copy.start()

    loads[0].wait()
    loads[1].wait()
    t = tok[...].astype(F32)
    scale = lax.rsqrt(jnp.mean(t * t, axis=-1, keepdims=True) + EPS)
    own_x = x.at[pl.ds(pl.multiple_of(h * rows, rows), rows), :]
    own_x[...] = (t * scale * gain[...]).astype(BF)
    loads[2].wait()

    pl.semaphore_wait(barrier, nh + ny + nz - 3)

    sends = []

    def go(copy):
        copy.start()
        sends.append(copy)

    def x_rows(p, core):
        return x.at[pl.ds(pl.multiple_of((p * nc + core) * rows, rows), rows), :]

    far_first = sorted(range(1, nx), key=lambda v: -min(v, nx - v))
    for d in far_first:
        go(rcopy(own_x, own_x, tok_ss.at[d], tok_rs.at[d], x_peer(d)[1]))
    if nc > 1:
        go(rcopy(own_x, own_x, pt_ss.at[0], pt_rs.at[0], partner))
    for d in range(1, ny):
        part = wt.at[0, z, y]
        go(rcopy(part, part, ow_ss.at[d, 0], ow_rs.at[d, 0], y_peer(d)[1]))
        part = wt.at[1, z, y]
        go(rcopy(part, part, ow_ss.at[d, 1], ow_rs.at[d, 1], z_peer(d)[1]))

    loads[3].wait()
    w[:, 0:128] = wqk[0].astype(F32).T.astype(BF)
    loads[4].wait()
    w[:, 256:384] = wqk[1].astype(F32).T.astype(BF)
    for copy in loads[5:]:
        copy.wait()

    row, col = iota((BLK, BLK), 0), iota((BLK, BLK), 1)
    lower = row >= col
    decb = jnp.broadcast_to(dec[...], (BLK, BLK))
    cum_col = jnp.sum(jnp.where(lower, decb, 0.0), axis=1, keepdims=True)
    dec_col = jnp.sum(jnp.where(row == col, decb, 0.0), axis=1, keepdims=True)
    cum_row = jnp.sum(jnp.where(row <= col, jnp.broadcast_to(dec_col, (BLK, BLK)), 0.0), axis=0, keepdims=True)
    cum_end = jnp.sum(dec[...], axis=1, keepdims=True)
    fade = jnp.exp(jnp.where(lower, cum_col - cum_row, -HUGE)) * (BLK ** (-0.5))
    key_weight = jnp.exp(cum_end - cum_col) * (BLK ** (-0.5))
    reach = jnp.exp(cum_col)
    sda[...] = jnp.broadcast_to(jnp.exp(cum_end), sda.shape)

    for d in sorted(range(1, nx), key=lambda v: min(v, nx - v)):
        p, dev = x_peer(nx - d)
        part = x_rows(p, c)
        rcopy(part, part, tok_ss.at[d], tok_rs.at[d], dev).wait_recv()
        if nc > 1:
            go(rcopy(part, part, pt_ss.at[d], pt_rs.at[d], partner))
    for d in range(1, ny):
        part = wt.at[0, z, y_peer(ny - d)[0]]
        rcopy(part, part, ow_ss.at[d, 0], ow_rs.at[d, 0], partner).wait_recv()
        part = wt.at[1, z_peer(nz - d)[0], y]
        rcopy(part, part, ow_ss.at[d, 1], ow_rs.at[d, 1], partner).wait_recv()

    def ow_hop(s, half, forward, arriving=False):
        place, peer = ((z, z_peer), (y, y_peer))[half]
        back = s if arriving else s - 1
        slot = lax.rem(place + (nz - back if forward else back), nz)
        ref = wt.at[0, slot] if half == 0 else wt.at[1, :, slot]
        ss, rs = (wf_ss, wf_rs) if forward else (wb_ss, wb_rs)
        return rcopy(ref, ref, ss.at[s - 1, half], rs.at[s - 1, half], peer(1 if forward else nz - 1)[1])

    def ow_start(s):
        for half in range(2):
            if s <= nf:
                go(ow_hop(s, half, True))
            if s <= nb:
                go(ow_hop(s, half, False))

    def ow_wait(s):
        for half in range(2):
            if s <= nf:
                ow_hop(s, half, True, True).wait_recv()
            if s <= nb:
                ow_hop(s, half, False, True).wait_recv()

    def ow_share(n, half):
        place = (z, y)[half]
        slot = lax.rem(place + (nz - (n + 1) // 2 if n % 2 else n // 2), nz)
        src, dst = (wt.at[0, slot], pwt.at[0, slot]) if half == 0 else (wt.at[1, :, slot], pwt.at[1, :, slot])
        return rcopy(src, dst, pw_ss.at[n, half], pw_rs.at[n, half], partner)

    def ow_pass(s):
        if nc > 1:
            for n in (2 * s - 1, 2 * s) if s else (0,):
                if n < nz:
                    for half in range(2):
                        ow_share(n, half).start()

    ow_start(1)
    ow_pass(0)

    if nc > 1:
        for d in range(nx):
            part = x_rows(lax.rem(fx + nx - d, nx), 1 - c)
            rcopy(part, part, pt_ss.at[d], pt_rs.at[d], partner).wait_recv()

    xs = x[...]
    kv = dot(xs, w[:, 0:256])
    kall[0:BLK, :] = kv[:, 0:128].astype(BF)
    vtall[:, 0:BLK] = kv[:, 128:256].T.astype(BF)

    def k_at(s):
        return kall.at[pl.ds(s * BLK, BLK), :]

    def v_at(s):
        return vtall.at[:, pl.ds(s * BLK, BLK)]

    def kv_hop(s, forward, part):
        source = RELAY[s]
        way = s - source if forward else nz - s + source
        if part == 2:
            src, dst = (source, s) if forward else ((nz - source) % nz, nz - s)
            return rcopy(qbuf.at[src], qbuf.at[dst], q_ss.at[dst], q_rs.at[dst], b_peer(way))
        if forward:
            src, dst, ss, rs = max(2 * source - 1, 0), 2 * s - 1, kf_ss, kf_rs
        else:
            src, dst, ss, rs = 2 * source, 2 * s, kb_ss, kb_rs
        at = (k_at, v_at)[part]
        return rcopy(at(src), at(dst), ss.at[s - 1, part], rs.at[s - 1, part], a_peer(way))

    def kv_start(source, part, ways=(True, False)):
        for s in range(nf, 0, -1):
            if RELAY[s] == source:
                for forward in ways:
                    if s <= (nf if forward else nb):
                        go(kv_hop(s, forward, part))

    def kv_advance(s):
        for part in range(3):
            for forward in (True, False):
                if s <= (nf if forward else nb):
                    kv_hop(s, forward, part).wait_recv()
                    kv_start(s, part, (forward,))

    kv_start(0, 0)
    kv_start(0, 1)

    rest = dot(xs, w[:, 256:768])
    qbuf[0] = (rest[:, 0:128].astype(BF).astype(F32) * (64 ** (-0.5))).T.astype(BF)
    kv_start(0, 2)

    rq, rk, rv = (rest[:, 128 * i : 128 * (i + 1)].astype(BF) for i in (1, 2, 3))
    keyed = (rk.astype(F32) * key_weight).T
    state = dot(keyed, rv.astype(F32), precision=HIGH)
    sa[...] = state.reshape(ny, sl, BLK).astype(BF)
    ra[pl.ds(y, 1)] = sa[pl.ds(y, 1)]
    rda[pl.ds(y, 1)] = sda[...].reshape(1, 1, BLK)
    for d in range(1, ny):
        p, dev = y_peer(d)
        go(rcopy(sa.at[p], ra.at[y], a_ss.at[d, 0], a_rs.at[d, 0], dev))
        go(rcopy(sda, rda.at[y], a_ss.at[d, 1], a_rs.at[d, 1], dev))

    kv_advance(1)
    scores = dot_nt(rq, rk) * fade
    inner = dot(scores.astype(BF), rv)
    reaching = rq.astype(F32) * reach

    ow_wait(1)
    ow_start(2)
    ow_pass(1)
    kv_advance(2)

    for d in range(1, ny):
        p, dev = y_peer(ny - d)
        rcopy(sa.at[p], ra.at[p], a_ss.at[d, 0], a_rs.at[d, 0], dev).wait_recv()
        rcopy(sda, rda.at[p], a_ss.at[d, 1], a_rs.at[d, 1], dev).wait_recv()
    total = ra[0].astype(F32)
    decay = rda[0]
    for i in range(1, ny):
        total = rda[i] * total + ra[i].astype(F32)
        decay = decay * rda[i]
    sb[...] = total.astype(BF)
    sdb[...] = decay
    rb[pl.ds(z, 1)] = jnp.zeros((1, sl, BLK), BF)
    rdb[pl.ds(z, 1)] = jnp.zeros((1, 1, BLK), F32)
    for d in range(1, nz):
        dev = z_peer(d)[1]
        go(rcopy(sb, rb.at[z], b_ss.at[d, 0], b_rs.at[d, 0], dev))
        go(rcopy(sdb, rdb.at[z], b_ss.at[d, 1], b_rs.at[d, 1], dev))

    krow, lane = iota((BLK, 2 * BLK), 0), iota((BLK, 2 * BLK), 1)
    qlane = jnp.where(lane >= BLK, lane - BLK, lane)
    steps = [0] + [(nz - (s + 1) // 2 if s % 2 else s // 2) for s in range(1, nz)]
    places = [a_place(lax.rem(a + step, nz)) for step in steps]
    key_blocks = [kz * ny + ky for kz, ky in places]
    top_half = row < 64

    def pair(i):
        return nz // 2 - i, lax.rem(nz // 2 + 1 + i, nz)

    def attend(i, lo, hi):
        places, wide = [], []
        for d in pair(i):
            places.append(b_place(lax.rem(b - d + nz, nz)))
            q = qbuf[d]
            zero = jnp.zeros_like(q)
            wide += [jnp.where(top_half, q, zero), jnp.where(top_half, zero, q)]
        blocks = [qz * ny + qy for qz, qy in places]
        s_all = dot(kall[lo * BLK : hi * BLK, :], jnp.concatenate(wide, axis=1))
        probs, peaks, totals = [], [], []
        for n in range(2):
            pieces = []
            for m in range(lo, hi):
                s = s_all[(m - lo) * BLK : (m - lo + 1) * BLK, n * 256 : (n + 1) * 256]
                if m == 0:
                    s = jnp.where(krow + key_blocks[0] * BLK <= qlane + blocks[n] * BLK, s, -HUGE)
                else:
                    s = s + jnp.where(key_blocks[m] < blocks[n], 0.0, -HUGE)
                pieces.append(s)
            s = jnp.concatenate(pieces, axis=0)
            peak = jnp.max(s, axis=0, keepdims=True)
            if lo == 0:
                peak = jnp.maximum(peak, FLOOR)
            else:
                peak = jnp.maximum(peak, early_stat[i, 0:1, n * 256 : (n + 1) * 256])
            p = jnp.exp(s - peak)
            peaks.append(peak)
            totals.append(jnp.sum(p, axis=0, keepdims=True))
            probs.append(p.astype(BF))
        sums = dot(vtall[:, lo * BLK : hi * BLK], jnp.concatenate(probs, axis=1))
        return sums, jnp.concatenate(peaks, axis=1), jnp.concatenate(totals, axis=1), places

    def attend_early(near, _):
        i = nz // 2 - 1 - near
        sums, peak, total, _ = attend(i, 0, early)
        early_sum[pl.ds(i, 1)] = sums[None]
        early_stat[pl.ds(i, 1)] = jnp.concatenate([peak, total], axis=0)[None]
        return 0

    def attend_late(i, _):
        first, second = pair(i)
        sums, peak, total, places = attend(i, early, nz)
        share = jnp.exp(early_stat[i, 0:1, :] - peak)
        total = total + share * early_stat[i, 1:2, :]
        sums = (sums + share * early_sum[i]).astype(BF)
        stat = jnp.concatenate([peak, total], axis=0)
        so[pl.ds(first, 1)] = sums[None, :, 0:256]
        so[pl.ds(second, 1)] = sums[None, :, 256:512]
        st[pl.ds(first, 1)] = stat[None, :, 0:256]
        st[pl.ds(second, 1)] = stat[None, :, 256:512]

        def send(d, place):
            dev = (*place, fx, c)
            rcopy(so.at[d], ro.at[d], r_ss.at[d, 0], r_rs.at[d, 0], dev).start()
            rcopy(st.at[d], rst.at[d], r_ss.at[d, 1], r_rs.at[d, 1], dev).start()

        send(first, places[0])

        @pl.when(i < nz // 2 - 1)
        def _():
            send(second, places[1])

        return 0

    pairs = nz // 2
    lax.fori_loop(0, min(2, pairs), attend_early, 0)
    for s in range(3, nf + 1):
        ow_wait(s - 1)
        ow_start(s)
        ow_pass(s - 1)
        kv_advance(s)
        lax.fori_loop(s - 1, s, attend_early, 0)

    for d in range(1, nz):
        p, dev = z_peer(nz - d)
        rcopy(sb, rb.at[p], b_ss.at[d, 0], b_rs.at[d, 0], dev).wait_recv()
        rcopy(sdb, rdb.at[p], b_ss.at[d, 1], b_rs.at[d, 1], dev).wait_recv()
    entry = init[0, pl.ds(pl.multiple_of(y * sl, sl), sl), :].astype(F32)
    for i in range(nz):
        entry = jnp.where(i < z, rdb[i] * entry + rb[i].astype(F32), entry)
    for i in range(ny):
        sc[i] = entry.astype(BF)
        entry = rda[i] * entry + ra[i].astype(F32)
    rc[pl.ds(y, 1)] = sc[pl.ds(y, 1)]
    for d in range(1, ny):
        p, dev = y_peer(d)
        rcopy(sc.at[p], rc.at[y], c_ss.at[d], c_rs.at[d], dev).start()

    lax.fori_loop(0, pairs, attend_late, 0)

    width = out_ref.shape[1]
    ow_wait(nf)
    ow_pass(nf)
    for half in range(2):
        wpair[half * BLK : (half + 1) * BLK, :] = wt[half].reshape(width, BLK).astype(F32).T.astype(BF)
    if nc > 1:
        for n in range(nz):
            for half in range(2):
                ow_share(n, half).wait_recv()
        for half in range(2):
            wpair[(2 + half) * BLK : (3 + half) * BLK, :] = pwt[half].reshape(width, BLK).astype(F32).T.astype(BF)

    for d in range(1, ny):
        p, dev = y_peer(ny - d)
        rcopy(sc.at[p], rc.at[p], c_ss.at[d], c_rs.at[d], dev).wait_recv()
    ret = inner + dot(reaching, rc[...].reshape(BLK, BLK).astype(F32), precision=HIGH)
    centre = ret - jnp.mean(ret, axis=-1, keepdims=True)
    ret_mix = (
        centre * lax.rsqrt(jnp.mean(centre * centre, axis=-1, keepdims=True) + EPS) * rgain[...]
    ).astype(BF)

    for d in range(1, ny):
        rcopy(so.at[d], ro.at[d], r_ss.at[d, 0], r_rs.at[d, 0], b_peer(d)).wait_recv()
        rcopy(st.at[d], rst.at[d], r_ss.at[d, 1], r_rs.at[d, 1], b_peer(d)).wait_recv()
    stats = [st[0]] + [rst[d] for d in range(1, ny)]
    top = stats[0][0:1]
    for one in stats[1:]:
        top = jnp.maximum(top, one[0:1])
    total = jnp.zeros_like(top)
    merged = jnp.zeros((BLK, 2 * BLK), F32)
    for d in range(ny):
        share = jnp.exp(stats[d][0:1] - top)
        total = total + share * stats[d][1:2]
        merged = merged + (so[0] if d == 0 else ro[d]).astype(F32) * share
    merged = merged / total
    diff = merged[:, 0:128] - lam_s[0] * merged[:, 128:256]
    diff = diff * lax.rsqrt(jnp.mean(diff * diff, axis=0, keepdims=True) + EPS)
    diff_mix = (diff.T * dgain[...]).astype(BF)

    mix = jnp.concatenate([ret_mix, diff_mix], axis=1)
    mixb[...] = mix.reshape(nx, nc, rows, 256)
    if nc > 1:
        swap = rcopy(mixb.at[:, 1 - c], pmix, mix_ss, mix_rs, partner)
        go(swap)
        swap.wait_recv()
        mine = mixb[:, pl.ds(c, 1)].reshape(nx * rows, 256)
        mix = jnp.concatenate([mine, pmix[...].reshape(nx * rows, 256)], axis=1)
    fs[...] = dot(mix, wpair[...]).astype(BF).reshape(nx, rows, width)
    for d in far_first:
        p, dev = x_peer(d)
        go(rcopy(fs.at[p], fr.at[d], f_ss.at[d], f_rs.at[d], dev))
    acc = fs[pl.ds(fx, 1)].reshape(rows, width).astype(F32)
    for d in range(1, nx):
        rcopy(fs.at[0], fr.at[d], f_ss.at[d], f_rs.at[d], x_peer(d)[1]).wait_recv()
        acc = acc + fr[d].astype(F32)
    out_ref[...] = acc.astype(BF)

    for copy in sends:
        copy.wait_send()
    if nc > 1:
        for n in range(nz):
            for half in range(2):
                ow_share(n, half).wait_send()
    for d in range(1, ny):
        p, dev = y_peer(d)
        rcopy(sc.at[p], rc.at[y], c_ss.at[d], c_rs.at[d], dev).wait_send()
        rcopy(so.at[d], ro.at[d], r_ss.at[d, 0], r_rs.at[d, 0], b_peer(d)).wait_send()
        rcopy(st.at[d], rst.at[d], r_ss.at[d, 1], r_rs.at[d, 1], b_peer(d)).wait_send()


def local(
    dims, tokens, in_gain, ret_query, ret_key, ret_value, decay_log, init_state, ret_gain,
    diff_query, diff_key, diff_value, diff_lambda, diff_gain, out_weight,
):
    nz, ny, nx, nc = dims
    nh = nx * nc
    rows, width = tokens.shape
    sl = BLK // ny
    nf, nb = nz // 2, nz - 1 - nz // 2
    dma = pltpu.SemaphoreType.DMA
    vm = pltpu.VMEM
    scratch = [
        vm((rows, width), BF), vm((1, width), F32), vm((1, BLK), F32), vm((1, BLK, BLK), BF),
        vm((1, BLK), F32), vm((1, BLK), F32), vm((2, BLK, width), BF), vm((width, 768), BF), vm((BLK, width), BF),
        vm((nz * BLK, BLK), BF), vm((BLK, nz * BLK), BF), vm((ny, BLK, BLK), BF),
        vm((ny, BLK, 2 * BLK), BF), vm((ny, 2, 2 * BLK), F32), vm((ny, BLK, 2 * BLK), BF), vm((ny, 2, 2 * BLK), F32),
        vm((ny, sl, BLK), BF), vm((1, BLK), F32), vm((ny, sl, BLK), BF), vm((ny, 1, BLK), F32),
        vm((sl, BLK), BF), vm((1, BLK), F32), vm((nz, sl, BLK), BF), vm((nz, 1, BLK), F32),
        vm((ny, sl, BLK), BF), vm((ny, sl, BLK), BF),
        vm((nz // 2, BLK, 4 * BLK), F32), vm((nz // 2, 2, 4 * BLK), F32),
        vm((2, nz, ny, 32, BLK), BF), vm((2, nz, ny, 32, BLK), BF), vm((2 * nc * BLK, width), BF),
        vm((nx, nc, rows, 2 * BLK), BF), vm((nx, rows, 2 * BLK), BF), vm((nx, rows, width), BF), vm((nx, rows, width), BF),
        dma((13,)), dma((nx,)), dma((nx,)), dma((nx,)), dma((nx,)), dma((ny, 2)), dma((ny, 2)),
        dma((nf, 2)), dma((nf, 2)), dma((max(nb, 1), 2)), dma((max(nb, 1), 2)), dma((ny,)), dma((ny,)),
        dma((ny, 2)), dma((ny, 2)), dma((nz, 2)), dma((nz, 2)), dma((ny,)), dma((ny,)),
        dma((ny, 2)), dma((ny, 2)), dma((nf, 2)), dma((nf, 2)), dma((max(nb, 1), 2)), dma((max(nb, 1), 2)),
        dma((nz, 2)), dma((nz, 2)), dma, dma, dma((nx,)), dma((nx,)),
    ]
    anyspec = pl.BlockSpec(memory_space=pl.ANY)
    smem = pl.BlockSpec(memory_space=pltpu.SMEM)
    return pl.pallas_call(
        functools.partial(kernel, dims),
        out_shape=jax.ShapeDtypeStruct((rows, width), BF),
        in_specs=[anyspec] * 11 + [smem] + [anyspec] * 2,
        out_specs=pl.BlockSpec(memory_space=pltpu.VMEM),
        scratch_shapes=scratch,
        compiler_params=pltpu.CompilerParams(
            collective_id=0, has_side_effects=True, vmem_limit_bytes=60 * 1024 * 1024
        ),
    )(
        tokens,
        in_gain.reshape(1, width),
        ret_query,
        ret_key,
        ret_value,
        decay_log,
        init_state,
        ret_gain.reshape(1, BLK),
        jnp.swapaxes(diff_query, 1, 2).reshape(BLK, width),
        jnp.swapaxes(diff_key, 1, 2).reshape(BLK, width),
        diff_value,
        diff_lambda,
        diff_gain.reshape(1, BLK),
        jnp.swapaxes(out_weight, 1, 2),
    )


def build(split):
    dims = tuple(split.shape[a] for a in SP_FS_TP)
    placed = (
        P(SP_FS_TP, None),
        P(),
        P(None, ("fs", "tp")),
        P(None, ("fs", "tp")),
        P(None, ("fs", "tp")),
        P(("fs", "tp"), SP),
        P(("fs", "tp"), None, None),
        P(("fs", "tp")),
        P(None, None, ("fs", "tp")),
        P(None, None, ("fs", "tp")),
        P(None, ("fs", "tp")),
        P(("fs", "tp")),
        P(("fs", "tp")),
        P(None, ("fs", "tp"), SP),
    )
    return jax.shard_map(
        functools.partial(local, dims), mesh=split, in_specs=placed, out_specs=P(SP_FS_TP, None), check_vma=False
    )


def solution(mesh):
    return build(Mesh(mesh.devices.reshape(8, 8, mesh.shape["fs"], mesh.shape["tp"]), SP_FS_TP))
```

```python
import functools

import jax
import jax.numpy as jnp
from jax import lax
from jax.experimental import pallas as pl
from jax.experimental.pallas import tpu as pltpu
from jax.sharding import Mesh
from jax.sharding import PartitionSpec as P

SP = ("sp_0", "sp_1")
SP_FS_TP = ("sp_0", "sp_1", "fs", "tp")
MESH = pl.DeviceIdType.MESH
EPS = 1e-06
HUGE = 1e30
FLOOR = -1e29
BLK = 128
RELAY = (None, 0, 1, 2, 3)
BF = jnp.bfloat16
F32 = jnp.float32
HIGH = lax.Precision.HIGHEST


def dot(a, b, **kw):
    return jnp.dot(a, b, preferred_element_type=F32, **kw)


def dot_nt(a, b):
    return lax.dot_general(a, b, (((1,), (1,)), ((), ())), preferred_element_type=F32)


def iota(shape, dim):
    return lax.broadcasted_iota(jnp.int32, shape, dim)


def kernel(
    dims,
    tok_h, gain_h, wrq_h, wrk_h, wrv_h, dec_h, init_h, rgain_h, wq_h, wk_h, wv_h, lam_s, dgain_h, ow_h,
    out_ref,
    tok, gain, dec, init, rgain, dgain, wqk, w, x,
    kall, vtall, qbuf, so, st, ro, rst,
    sa, sda, ra, rda, sb, sdb, rb, rdb, sc, rc,
    early_sum, early_stat, wt, pwt, wpair, mixb, pmix, fs, fr,
    in_sem, tok_ss, tok_rs, pt_ss, pt_rs, ow_ss, ow_rs, kf_ss, kf_rs, kb_ss, kb_rs, q_ss, q_rs,
    a_ss, a_rs, b_ss, b_rs, c_ss, c_rs, r_ss, r_rs, wf_ss, wf_rs, wb_ss, wb_rs, pw_ss, pw_rs, mix_ss, mix_rs, f_ss, f_rs,
):
    nz, ny, nx, nc = dims
    nh = nx * nc
    rows = BLK // nh
    sl = BLK // ny
    nf, nb = nz // 2, nz - 1 - nz // 2
    early = 5 if nz > 5 else 3
    z, y = lax.axis_index("sp_0"), lax.axis_index("sp_1")
    fx, c = lax.axis_index("fs"), lax.axis_index("tp")
    h = fx * nc + c

    def head_peer(d):
        p = lax.rem(h + d, nh)
        return p, (z, y, p // nc, lax.rem(p, nc))

    a, b = (1 - c) * z + c * y, (1 - c) * y + c * z

    def a_place(p):
        return z + (1 - c) * (p - a), y + c * (p - a)

    def b_place(p):
        return z + c * (p - b), y + (1 - c) * (p - b)

    def a_peer(d):
        return (*a_place(lax.rem(a + d, nz)), fx, c)

    def b_peer(d):
        return (*b_place(lax.rem(b + d, nz)), fx, c)

    def x_peer(d):
        p = lax.rem(fx + d, nx)
        return p, (z, y, p, c)

    partner = (z, y, fx, 1 - c)

    def y_peer(d):
        p = lax.rem(y + d, ny)
        return p, (z, p, fx, c)

    def z_peer(d):
        p = lax.rem(z + d, nz)
        return p, (p, y, fx, c)

    def rcopy(src, dst, ss, rs, dev):
        return pltpu.make_async_remote_copy(
            src_ref=src, dst_ref=dst, send_sem=ss, recv_sem=rs, device_id=dev, device_id_type=MESH
        )

    barrier = pltpu.get_barrier_semaphore()
    for d in range(1, nh):
        pl.semaphore_signal(barrier, inc=1, device_id=head_peer(d)[1], device_id_type=MESH)
    for d in range(1, ny):
        pl.semaphore_signal(barrier, inc=1, device_id=y_peer(d)[1], device_id_type=MESH)
    for d in range(1, nz):
        pl.semaphore_signal(barrier, inc=1, device_id=z_peer(d)[1], device_id_type=MESH)

    inputs = [
        (tok_h, tok), (gain_h, gain), (ow_h, wt.at[:, z, y]), (wk_h, wqk.at[0]), (wq_h, wqk.at[1]),
        (wv_h, w.at[:, pl.ds(128, 128)]), (wrq_h, w.at[:, pl.ds(384, 128)]),
        (wrk_h, w.at[:, pl.ds(512, 128)]), (wrv_h, w.at[:, pl.ds(640, 128)]),
        (dec_h, dec), (init_h, init), (rgain_h, rgain), (dgain_h, dgain),
    ]
    loads = [pltpu.make_async_copy(s, t, in_sem.at[i]) for i, (s, t) in enumerate(inputs)]
    for copy in loads:
        copy.start()

    loads[0].wait()
    loads[1].wait()
    t = tok[...].astype(F32)
    scale = lax.rsqrt(jnp.mean(t * t, axis=-1, keepdims=True) + EPS)
    own_x = x.at[pl.ds(pl.multiple_of(h * rows, rows), rows), :]
    own_x[...] = (t * scale * gain[...]).astype(BF)

    pl.semaphore_wait(barrier, nh + ny + nz - 3)

    sends = []

    def go(copy):
        copy.start()
        sends.append(copy)

    def x_rows(p, core):
        return x.at[pl.ds(pl.multiple_of((p * nc + core) * rows, rows), rows), :]

    far_first = sorted(range(1, nx), key=lambda v: -min(v, nx - v))
    for d in far_first:
        go(rcopy(own_x, own_x, tok_ss.at[d], tok_rs.at[d], x_peer(d)[1]))
    if nc > 1:
        go(rcopy(own_x, own_x, pt_ss.at[0], pt_rs.at[0], partner))
    loads[2].wait()
    for d in range(1, ny):
        part = wt.at[0, z, y]
        go(rcopy(part, part, ow_ss.at[d, 0], ow_rs.at[d, 0], y_peer(d)[1]))
        part = wt.at[1, z, y]
        go(rcopy(part, part, ow_ss.at[d, 1], ow_rs.at[d, 1], z_peer(d)[1]))

    loads[3].wait()
    w[:, 0:128] = wqk[0].astype(F32).T.astype(BF)
    loads[4].wait()
    w[:, 256:384] = wqk[1].astype(F32).T.astype(BF)
    for copy in loads[5:]:
        copy.wait()

    row, col = iota((BLK, BLK), 0), iota((BLK, BLK), 1)
    lower = row >= col
    decb = jnp.broadcast_to(dec[...], (BLK, BLK))
    cum_col = jnp.sum(jnp.where(lower, decb, 0.0), axis=1, keepdims=True)
    dec_col = jnp.sum(jnp.where(row == col, decb, 0.0), axis=1, keepdims=True)
    cum_row = jnp.sum(jnp.where(row <= col, jnp.broadcast_to(dec_col, (BLK, BLK)), 0.0), axis=0, keepdims=True)
    cum_end = jnp.sum(dec[...], axis=1, keepdims=True)
    fade = jnp.exp(jnp.where(lower, cum_col - cum_row, -HUGE)) * (BLK ** (-0.5))
    key_weight = jnp.exp(cum_end - cum_col) * (BLK ** (-0.5))
    reach = jnp.exp(cum_col)
    sda[...] = jnp.broadcast_to(jnp.exp(cum_end), sda.shape)

    for d in sorted(range(1, nx), key=lambda v: min(v, nx - v)):
        p, dev = x_peer(nx - d)
        part = x_rows(p, c)
        rcopy(part, part, tok_ss.at[d], tok_rs.at[d], dev).wait_recv()
        if nc > 1:
            go(rcopy(part, part, pt_ss.at[d], pt_rs.at[d], partner))
    for d in range(1, ny):
        part = wt.at[0, z, y_peer(ny - d)[0]]
        rcopy(part, part, ow_ss.at[d, 0], ow_rs.at[d, 0], partner).wait_recv()
        part = wt.at[1, z_peer(nz - d)[0], y]
        rcopy(part, part, ow_ss.at[d, 1], ow_rs.at[d, 1], partner).wait_recv()

    def ow_hop(s, half, forward, arriving=False):
        place, peer = ((z, z_peer), (y, y_peer))[half]
        back = s if arriving else s - 1
        slot = lax.rem(place + (nz - back if forward else back), nz)
        ref = wt.at[0, slot] if half == 0 else wt.at[1, :, slot]
        ss, rs = (wf_ss, wf_rs) if forward else (wb_ss, wb_rs)
        return rcopy(ref, ref, ss.at[s - 1, half], rs.at[s - 1, half], peer(1 if forward else nz - 1)[1])

    def ow_start(s):
        for half in range(2):
            if s <= nf:
                go(ow_hop(s, half, True))
            if s <= nb:
                go(ow_hop(s, half, False))

    def ow_wait(s):
        for half in range(2):
            if s <= nf:
                ow_hop(s, half, True, True).wait_recv()
            if s <= nb:
                ow_hop(s, half, False, True).wait_recv()

    def ow_share(n, half):
        place = (z, y)[half]
        slot = lax.rem(place + (nz - (n + 1) // 2 if n % 2 else n // 2), nz)
        src, dst = (wt.at[0, slot], pwt.at[0, slot]) if half == 0 else (wt.at[1, :, slot], pwt.at[1, :, slot])
        return rcopy(src, dst, pw_ss.at[n, half], pw_rs.at[n, half], partner)

    def ow_pass(s):
        if nc > 1:
            for n in (2 * s - 1, 2 * s) if s else (0,):
                if n < nz:
                    for half in range(2):
                        ow_share(n, half).start()

    ow_start(1)
    ow_pass(0)

    if nc > 1:
        for d in range(nx):
            part = x_rows(lax.rem(fx + nx - d, nx), 1 - c)
            rcopy(part, part, pt_ss.at[d], pt_rs.at[d], partner).wait_recv()

    xs = x[...]
    kv = dot(xs, w[:, 0:256])
    kall[0:BLK, :] = kv[:, 0:128].astype(BF)
    vtall[:, 0:BLK] = kv[:, 128:256].T.astype(BF)

    def k_at(s):
        return kall.at[pl.ds(s * BLK, BLK), :]

    def v_at(s):
        return vtall.at[:, pl.ds(s * BLK, BLK)]

    def kv_hop(s, forward, part):
        source = RELAY[s]
        way = s - source if forward else nz - s + source
        if part == 2:
            src, dst = (source, s) if forward else ((nz - source) % nz, nz - s)
            return rcopy(qbuf.at[src], qbuf.at[dst], q_ss.at[dst], q_rs.at[dst], b_peer(way))
        if forward:
            src, dst, ss, rs = max(2 * source - 1, 0), 2 * s - 1, kf_ss, kf_rs
        else:
            src, dst, ss, rs = 2 * source, 2 * s, kb_ss, kb_rs
        at = (k_at, v_at)[part]
        return rcopy(at(src), at(dst), ss.at[s - 1, part], rs.at[s - 1, part], a_peer(way))

    def kv_start(source, part, ways=(True, False)):
        for s in range(nf, 0, -1):
            if RELAY[s] == source:
                for forward in ways:
                    if s <= (nf if forward else nb):
                        go(kv_hop(s, forward, part))

    def kv_advance(s):
        for part in range(3):
            for forward in (True, False):
                if s <= (nf if forward else nb):
                    kv_hop(s, forward, part).wait_recv()
                    kv_start(s, part, (forward,))

    kv_start(0, 0)
    kv_start(0, 1)

    rest = dot(xs, w[:, 256:768])
    qbuf[0] = (rest[:, 0:128].astype(BF).astype(F32) * (64 ** (-0.5))).T.astype(BF)
    kv_start(0, 2)

    rq, rk, rv = (rest[:, 128 * i : 128 * (i + 1)].astype(BF) for i in (1, 2, 3))
    keyed = (rk.astype(F32) * key_weight).T
    state = dot(keyed, rv.astype(F32), precision=HIGH)
    sa[...] = state.reshape(ny, sl, BLK).astype(BF)
    ra[pl.ds(y, 1)] = sa[pl.ds(y, 1)]
    rda[pl.ds(y, 1)] = sda[...].reshape(1, 1, BLK)
    for d in range(1, ny):
        p, dev = y_peer(d)
        go(rcopy(sa.at[p], ra.at[y], a_ss.at[d, 0], a_rs.at[d, 0], dev))
        go(rcopy(sda, rda.at[y], a_ss.at[d, 1], a_rs.at[d, 1], dev))

    kv_advance(1)
    scores = dot_nt(rq, rk) * fade
    inner = dot(scores.astype(BF), rv)
    reaching = rq.astype(F32) * reach

    ow_wait(1)
    ow_start(2)
    ow_pass(1)
    kv_advance(2)

    for d in range(1, ny):
        p, dev = y_peer(ny - d)
        rcopy(sa.at[p], ra.at[p], a_ss.at[d, 0], a_rs.at[d, 0], dev).wait_recv()
        rcopy(sda, rda.at[p], a_ss.at[d, 1], a_rs.at[d, 1], dev).wait_recv()
    total = ra[0].astype(F32)
    decay = rda[0]
    for i in range(1, ny):
        total = rda[i] * total + ra[i].astype(F32)
        decay = decay * rda[i]
    sb[...] = total.astype(BF)
    sdb[...] = decay
    rb[pl.ds(z, 1)] = jnp.zeros((1, sl, BLK), BF)
    rdb[pl.ds(z, 1)] = jnp.zeros((1, 1, BLK), F32)
    for d in range(1, nz):
        dev = z_peer(d)[1]
        go(rcopy(sb, rb.at[z], b_ss.at[d, 0], b_rs.at[d, 0], dev))
        go(rcopy(sdb, rdb.at[z], b_ss.at[d, 1], b_rs.at[d, 1], dev))

    krow, lane = iota((BLK, 2 * BLK), 0), iota((BLK, 2 * BLK), 1)
    qlane = jnp.where(lane >= BLK, lane - BLK, lane)
    steps = [0] + [(nz - (s + 1) // 2 if s % 2 else s // 2) for s in range(1, nz)]
    places = [a_place(lax.rem(a + step, nz)) for step in steps]
    key_blocks = [kz * ny + ky for kz, ky in places]
    top_half = row < 64

    def pair(i):
        return nz // 2 - i, (nz // 2 + 1 + i) % nz

    def attend(i, lo, hi):
        places, wide = [], []
        for d in pair(i):
            places.append(b_place(lax.rem(b - d + nz, nz)))
            q = qbuf[d]
            zero = jnp.zeros_like(q)
            wide += [jnp.where(top_half, q, zero), jnp.where(top_half, zero, q)]
        blocks = [qz * ny + qy for qz, qy in places]
        s_all = dot(kall[lo * BLK : hi * BLK, :], jnp.concatenate(wide, axis=1))
        probs, peaks, totals = [], [], []
        for n in range(2):
            pieces = []
            for m in range(lo, hi):
                s = s_all[(m - lo) * BLK : (m - lo + 1) * BLK, n * 256 : (n + 1) * 256]
                if m == 0:
                    s = jnp.where(krow + key_blocks[0] * BLK <= qlane + blocks[n] * BLK, s, -HUGE)
                else:
                    s = s + jnp.where(key_blocks[m] < blocks[n], 0.0, -HUGE)
                pieces.append(s)
            s = jnp.concatenate(pieces, axis=0)
            peak = jnp.max(s, axis=0, keepdims=True)
            if lo == 0:
                peak = jnp.maximum(peak, FLOOR)
            else:
                peak = jnp.maximum(peak, early_stat[i, 0:1, n * 256 : (n + 1) * 256])
            p = jnp.exp(s - peak)
            peaks.append(peak)
            totals.append(jnp.sum(p, axis=0, keepdims=True))
            probs.append(p.astype(BF))
        sums = dot(vtall[:, lo * BLK : hi * BLK], jnp.concatenate(probs, axis=1))
        return sums, jnp.concatenate(peaks, axis=1), jnp.concatenate(totals, axis=1), places

    def absorb(i, lo, hi):
        first, second = pair(i)
        sums, peak, total, places = attend(i, lo, hi)
        if lo:
            share = jnp.exp(early_stat[i, 0:1, :] - peak)
            total = total + share * early_stat[i, 1:2, :]
            sums = sums + share * early_sum[i]
        stat = jnp.concatenate([peak, total], axis=0)
        if hi < nz:
            early_sum[i] = sums
            early_stat[i] = stat
            return
        sums = sums.astype(BF)
        so[pl.ds(first, 1)] = sums[None, :, 0:256]
        so[pl.ds(second, 1)] = sums[None, :, 256:512]
        st[pl.ds(first, 1)] = stat[None, :, 0:256]
        st[pl.ds(second, 1)] = stat[None, :, 256:512]

        def send(d, place):
            dev = (*place, fx, c)
            rcopy(so.at[d], ro.at[d], r_ss.at[d, 0], r_rs.at[d, 0], dev).start()
            rcopy(st.at[d], rst.at[d], r_ss.at[d, 1], r_rs.at[d, 1], dev).start()

        send(first, places[0])

        if second:
            send(second, places[1])

    pairs = nz // 2
    middle = nz - 1 if nf > 2 else early
    absorb(pairs - 1, 0, early)
    if nf > 2:
        absorb(pairs - 2, 0, early)
        ow_wait(2)
        ow_start(3)
        ow_pass(2)
        kv_advance(3)
        absorb(pairs - 3, 0, middle)
        ow_wait(3)
        ow_start(4)
        ow_pass(3)
        absorb(pairs - 1, early, middle)
        absorb(pairs - 2, early, middle)

    for d in range(1, nz):
        p, dev = z_peer(nz - d)
        rcopy(sb, rb.at[p], b_ss.at[d, 0], b_rs.at[d, 0], dev).wait_recv()
        rcopy(sdb, rdb.at[p], b_ss.at[d, 1], b_rs.at[d, 1], dev).wait_recv()
    entry = init[0, pl.ds(pl.multiple_of(y * sl, sl), sl), :].astype(F32)
    for i in range(nz):
        entry = jnp.where(i < z, rdb[i] * entry + rb[i].astype(F32), entry)
    for i in range(ny):
        sc[i] = entry.astype(BF)
        entry = rda[i] * entry + ra[i].astype(F32)
    rc[pl.ds(y, 1)] = sc[pl.ds(y, 1)]
    for d in range(1, ny):
        p, dev = y_peer(d)
        rcopy(sc.at[p], rc.at[y], c_ss.at[d], c_rs.at[d], dev).start()

    if nf > 2:
        kv_advance(4)
    absorb(0, 0, nz)
    for i in range(1, pairs):
        absorb(i, middle, nz)

    width = out_ref.shape[1]
    ow_wait(nf)
    ow_pass(nf)
    for half in range(2):
        wpair[half * BLK : (half + 1) * BLK, :] = wt[half].reshape(width, BLK).astype(F32).T.astype(BF)
    if nc > 1:
        for n in range(nz):
            for half in range(2):
                ow_share(n, half).wait_recv()
        for half in range(2):
            wpair[(2 + half) * BLK : (3 + half) * BLK, :] = pwt[half].reshape(width, BLK).astype(F32).T.astype(BF)

    for d in range(1, ny):
        p, dev = y_peer(ny - d)
        rcopy(sc.at[p], rc.at[p], c_ss.at[d], c_rs.at[d], dev).wait_recv()
    ret = inner + dot(reaching, rc[...].reshape(BLK, BLK).astype(F32), precision=HIGH)
    centre = ret - jnp.mean(ret, axis=-1, keepdims=True)
    ret_mix = (
        centre * lax.rsqrt(jnp.mean(centre * centre, axis=-1, keepdims=True) + EPS) * rgain[...]
    ).astype(BF)

    for d in range(1, ny):
        rcopy(so.at[d], ro.at[d], r_ss.at[d, 0], r_rs.at[d, 0], b_peer(d)).wait_recv()
        rcopy(st.at[d], rst.at[d], r_ss.at[d, 1], r_rs.at[d, 1], b_peer(d)).wait_recv()
    stats = [st[0]] + [rst[d] for d in range(1, ny)]
    top = stats[0][0:1]
    for one in stats[1:]:
        top = jnp.maximum(top, one[0:1])
    total = jnp.zeros_like(top)
    merged = jnp.zeros((BLK, 2 * BLK), F32)
    for d in range(ny):
        share = jnp.exp(stats[d][0:1] - top)
        total = total + share * stats[d][1:2]
        merged = merged + (so[0] if d == 0 else ro[d]).astype(F32) * share
    merged = merged / total
    diff = merged[:, 0:128] - lam_s[0] * merged[:, 128:256]
    diff = diff * lax.rsqrt(jnp.mean(diff * diff, axis=0, keepdims=True) + EPS)
    diff_mix = (diff.T * dgain[...]).astype(BF)

    mix = jnp.concatenate([ret_mix, diff_mix], axis=1)
    mixb[...] = mix.reshape(nx, nc, rows, 256)
    if nc > 1:
        swap = rcopy(mixb.at[:, 1 - c], pmix, mix_ss, mix_rs, partner)
        go(swap)
        swap.wait_recv()
        mine = mixb[:, pl.ds(c, 1)].reshape(nx * rows, 256)
        mix = jnp.concatenate([mine, pmix[...].reshape(nx * rows, 256)], axis=1)
    fs[...] = dot(mix, wpair[...]).astype(BF).reshape(nx, rows, width)
    for d in far_first:
        p, dev = x_peer(d)
        go(rcopy(fs.at[p], fr.at[d], f_ss.at[d], f_rs.at[d], dev))
    acc = fs[pl.ds(fx, 1)].reshape(rows, width).astype(F32)
    for d in range(1, nx):
        rcopy(fs.at[0], fr.at[d], f_ss.at[d], f_rs.at[d], x_peer(d)[1]).wait_recv()
        acc = acc + fr[d].astype(F32)
    out_ref[...] = acc.astype(BF)

    for copy in sends:
        copy.wait_send()
    if nc > 1:
        for n in range(nz):
            for half in range(2):
                ow_share(n, half).wait_send()
    for d in range(1, ny):
        p, dev = y_peer(d)
        rcopy(sc.at[p], rc.at[y], c_ss.at[d], c_rs.at[d], dev).wait_send()
        rcopy(so.at[d], ro.at[d], r_ss.at[d, 0], r_rs.at[d, 0], b_peer(d)).wait_send()
        rcopy(st.at[d], rst.at[d], r_ss.at[d, 1], r_rs.at[d, 1], b_peer(d)).wait_send()


def local(
    dims, tokens, in_gain, ret_query, ret_key, ret_value, decay_log, init_state, ret_gain,
    diff_query, diff_key, diff_value, diff_lambda, diff_gain, out_weight,
):
    nz, ny, nx, nc = dims
    nh = nx * nc
    rows, width = tokens.shape
    sl = BLK // ny
    nf, nb = nz // 2, nz - 1 - nz // 2
    dma = pltpu.SemaphoreType.DMA
    vm = pltpu.VMEM
    scratch = [
        vm((rows, width), BF), vm((1, width), F32), vm((1, BLK), F32), vm((1, BLK, BLK), BF),
        vm((1, BLK), F32), vm((1, BLK), F32), vm((2, BLK, width), BF), vm((width, 768), BF), vm((BLK, width), BF),
        vm((nz * BLK, BLK), BF), vm((BLK, nz * BLK), BF), vm((ny, BLK, BLK), BF),
        vm((ny, BLK, 2 * BLK), BF), vm((ny, 2, 2 * BLK), F32), vm((ny, BLK, 2 * BLK), BF), vm((ny, 2, 2 * BLK), F32),
        vm((ny, sl, BLK), BF), vm((1, BLK), F32), vm((ny, sl, BLK), BF), vm((ny, 1, BLK), F32),
        vm((sl, BLK), BF), vm((1, BLK), F32), vm((nz, sl, BLK), BF), vm((nz, 1, BLK), F32),
        vm((ny, sl, BLK), BF), vm((ny, sl, BLK), BF),
        vm((nz // 2, BLK, 4 * BLK), F32), vm((nz // 2, 2, 4 * BLK), F32),
        vm((2, nz, ny, 32, BLK), BF), vm((2, nz, ny, 32, BLK), BF), vm((2 * nc * BLK, width), BF),
        vm((nx, nc, rows, 2 * BLK), BF), vm((nx, rows, 2 * BLK), BF), vm((nx, rows, width), BF), vm((nx, rows, width), BF),
        dma((13,)), dma((nx,)), dma((nx,)), dma((nx,)), dma((nx,)), dma((ny, 2)), dma((ny, 2)),
        dma((nf, 2)), dma((nf, 2)), dma((max(nb, 1), 2)), dma((max(nb, 1), 2)), dma((ny,)), dma((ny,)),
        dma((ny, 2)), dma((ny, 2)), dma((nz, 2)), dma((nz, 2)), dma((ny,)), dma((ny,)),
        dma((ny, 2)), dma((ny, 2)), dma((nf, 2)), dma((nf, 2)), dma((max(nb, 1), 2)), dma((max(nb, 1), 2)),
        dma((nz, 2)), dma((nz, 2)), dma, dma, dma((nx,)), dma((nx,)),
    ]
    anyspec = pl.BlockSpec(memory_space=pl.ANY)
    smem = pl.BlockSpec(memory_space=pltpu.SMEM)
    return pl.pallas_call(
        functools.partial(kernel, dims),
        out_shape=jax.ShapeDtypeStruct((rows, width), BF),
        in_specs=[anyspec] * 11 + [smem] + [anyspec] * 2,
        out_specs=pl.BlockSpec(memory_space=pltpu.VMEM),
        scratch_shapes=scratch,
        compiler_params=pltpu.CompilerParams(
            collective_id=0, has_side_effects=True, vmem_limit_bytes=60 * 1024 * 1024
        ),
    )(
        tokens,
        in_gain.reshape(1, width),
        ret_query,
        ret_key,
        ret_value,
        decay_log,
        init_state,
        ret_gain.reshape(1, BLK),
        jnp.swapaxes(diff_query, 1, 2).reshape(BLK, width),
        jnp.swapaxes(diff_key, 1, 2).reshape(BLK, width),
        diff_value,
        diff_lambda,
        diff_gain.reshape(1, BLK),
        jnp.swapaxes(out_weight, 1, 2),
    )


def build(split):
    dims = tuple(split.shape[a] for a in SP_FS_TP)
    placed = (
        P(SP_FS_TP, None),
        P(),
        P(None, ("fs", "tp")),
        P(None, ("fs", "tp")),
        P(None, ("fs", "tp")),
        P(("fs", "tp"), SP),
        P(("fs", "tp"), None, None),
        P(("fs", "tp")),
        P(None, None, ("fs", "tp")),
        P(None, None, ("fs", "tp")),
        P(None, ("fs", "tp")),
        P(("fs", "tp")),
        P(("fs", "tp")),
        P(None, ("fs", "tp"), SP),
    )
    return jax.shard_map(
        functools.partial(local, dims), mesh=split, in_specs=placed, out_specs=P(SP_FS_TP, None), check_vma=False
    )


def solution(mesh):
    return build(Mesh(mesh.devices.reshape(8, 8, mesh.shape["fs"], mesh.shape["tp"]), SP_FS_TP))
```
